256 devices in a mesh: sp: 16 (over y, x), tp: 16 (over z, core).
Axes of the slice: x: 4, y: 4, z: 8, core: 2. Of those that a mesh axis runs over, the one named last changes fastest.
Arguments:
- conv_value: bfloat16 [1024, 16384], P('tp', 'sp'), may hold values from -6 to 6
- conv_gate: bfloat16 [1024, 16384], P('tp', 'sp'), may hold values from -6 to 6
- conv_taps: float32 [1024, 31], P('tp'), may hold values from -2.2 to 2.2
- norm_gain: float32 [1024], replicated, may hold values from 0.1 to 1.9
- norm_bias: float32 [1024], replicated, may hold values from -3 to 3
- out_weight: bfloat16 [1024, 2048], replicated, may hold values from -0.1875 to 0.1875
- stream: bfloat16 [16384, 2048], P(('sp', 'tp')), may hold values from -6 to 6
- routes: int32 [16384, 2], P(('sp', 'tp')), may hold values from 0 to 15, all different within a row; in each aligned block of 64 rows (0 to 63, 64 to 127, ...) at most 8 rows name the same one
- route_weights: float32 [16384, 2], P(('sp', 'tp')), may hold values from 0.2 to 1
- expert_gain: float32 [2048], replicated, may hold values from 0.1 to 1.9
- expert_gate: bfloat16 [16, 2048, 7168], P('sp', None, 'tp'), may hold values from -0.125 to 0.125
- expert_up: bfloat16 [16, 2048, 7168], P('sp', None, 'tp'), may hold values from -0.125 to 0.125
- expert_down: bfloat16 [16, 7168, 2048], P('sp', 'tp'), may hold values from -0.0625 to 0.0625
Outputs:
- mixed: bfloat16 [16384, 2048], P(('sp', 'tp'))
The draws below stay inside these ranges and needn't reach their ends.
Inputs may be any that keep to these rules, and one draw needn't show every extreme that they name: `routes`: within each device's 64 rows every expert is named exactly 8 times; a row names distinct experts.
All inputs are finite; a program needn't handle non-finite values.
Results may differ from the reference program's by a relative error of at most 0.014.
Values may be sent and summed in bfloat16 or wider, within the bound.
A program may use at most 64 MiB of HBM per device.

```python
import math
import jax
import jax.numpy as jnp
import numpy as np
from jax import lax

D = 2048
CONV_CH = 1024
KERNEL = 31
FF_E = 7168
TOP = 2
TOK_DEV = 64
EXPERTS = 16
CAP = 8
TOKENS = 16384
N_TP = 16


def draw_conv_taps(key, part):
    base = jnp.clip(jax.random.normal(key, (CONV_CH, KERNEL), jnp.float32), -4.0, 4.0)
    scales = jnp.exp(jnp.linspace(math.log(0.5), math.log(3.0), CONV_CH))
    return (base * scales[:, None] * KERNEL ** (-0.5)).astype(jnp.float32)


def block_levels(stream_key, shape, pieces, low, high):
    factor_of, own = 1.0, jax.random.fold_in(stream_key, 6)
    for axis_at, shards_of in pieces:
        steps = jnp.exp(jax.random.uniform(jax.random.fold_in(own, axis_at), (shards_of,), jnp.float32, low / len(pieces), high / len(pieces)))
        factor_of = factor_of * jnp.repeat(steps, shape[axis_at] // shards_of).reshape([-1 if axis == axis_at else 1 for axis in range(len(shape))])
    return factor_of


def routed_block(stream_key, own, number, rows, count, top, bound, lean):
    ranking = jax.random.permutation(stream_key, count)
    heavy_load, usual = shares(count, rows * top, bound, lean, True), shares(count, rows * top, bound, lean, False)
    places = jnp.arange(count)

    def named(tallies, rotation):
        used = int((tallies > 0).sum())
        fixed = max(1, used // 4)
        moved = fixed + (places - fixed + rotation * (used - fixed)) % max(1, count - fixed)
        return jnp.zeros((count,), jnp.int32).at[ranking[jnp.where(places < fixed, places, moved)]].set(jnp.asarray(tallies, jnp.int32))

    tallies = jnp.where(number % 4 == 0, named(heavy_load, number // 4), named(usual, number - number // 4 - 1))
    mixed = jax.random.permutation(jax.random.fold_in(own, 3), count)
    donor, taker = mixed[0:count // 2 * 2:2], mixed[1:count // 2 * 2:2]
    margin = jnp.minimum(tallies[donor] - 1, bound - tallies[taker]) // 2
    margin = jnp.where((donor == ranking[0]) | (taker == ranking[0]) | (tallies[taker] == 0), 0, jnp.maximum(margin, 0))
    moved = jax.random.randint(jax.random.fold_in(own, 4), (count // 2,), 0, 1 << 20) % (margin + 1)
    tallies = tallies.at[donor].add(-moved).at[taker].add(moved)
    members = jnp.searchsorted(jnp.cumsum(tallies), jnp.arange(rows * top), side="right").astype(jnp.int32)
    listing = members.reshape(top, rows).T
    listing = listing[jax.random.permutation(jax.random.fold_in(own, 1), rows)]
    rotation = jax.random.randint(jax.random.fold_in(own, 2), (rows, 1), 0, top)
    return jnp.take_along_axis(listing, (jnp.arange(top)[None, :] + rotation) % top, axis=1)


def shares(number_of, total, bound, lean, full):
    loads = [(1 << 20) // math.isqrt(grade ** lean) + 1 for grade in range(1, number_of + 1)]
    largest = bound if full else min(bound, max(-(-total // number_of), total * loads[0] // sum(loads)))
    least = 1 if total - largest >= number_of - 1 else 0
    given, rest = [largest] + [least] * (number_of - 1), total - largest - least * (number_of - 1)
    while rest > 0:
        candidates = [i for i in range(1, number_of) if given[i] < largest] or [i for i in range(1, number_of) if given[i] < bound]
        pool, left = sum([loads[i] for i in candidates]), rest
        for i in candidates:
            extra = min(bound - given[i], max(1, left * loads[i] // pool), rest)
            given[i] = given[i] + extra
            rest = rest - extra
    return np.array(given)


def normal_values(own_key, shape, scale, limit, pieces=(), kind=jnp.bfloat16):
    drawn = scale * jax.random.normal(own_key, shape, jnp.float32)
    if pieces:
        drawn = drawn * block_levels(own_key, shape, pieces, -0.22, 0.18)
    return jnp.clip(drawn, -limit, limit).astype(kind)


def setup_inputs(seed: int = 0) -> dict:
    key_of = jax.random.split(jax.random.key(seed), 14)
    conv_value = normal_values(key_of[0], (CONV_CH, TOKENS), 1.0, 6.0, ((0, 16), (1, 16)))
    conv_gate = normal_values(key_of[1], (CONV_CH, TOKENS), 1.5, 6.0, ((0, 16), (1, 16)))
    conv_taps = draw_conv_taps(jax.random.fold_in(key_of[13], 71), 0)
    norm_gain = jnp.clip(1.0 + 0.18 * jax.random.normal(key_of[3], (CONV_CH,), jnp.float32), 0.1, 1.9)
    norm_bias = normal_values(key_of[4], (CONV_CH,), 0.5, 3.0, (), jnp.float32)
    out_weight = normal_values(key_of[5], (CONV_CH, D), CONV_CH ** -0.5, 0.1875)
    stream = normal_values(key_of[6], (TOKENS, D), 1.0, 6.0, ((0, 256),))
    routes_keys = jax.random.split(jax.random.fold_in(key_of[7], 1), TOKENS // TOK_DEV)
    routes_turns = jax.random.permutation(jax.random.fold_in(key_of[7], 3), TOKENS // TOK_DEV)
    routes = jax.vmap(lambda own, number: routed_block(jax.random.fold_in(key_of[7], 2), own, number, TOK_DEV, EXPERTS, TOP, CAP, 0))(routes_keys, routes_turns).reshape((TOKENS, TOP))
    route_weights = jnp.clip(0.2 + 0.8 * jax.random.uniform(key_of[8], (TOKENS, TOP), jnp.float32) ** block_levels(key_of[8], (TOKENS, TOP), ((0, 256),), -0.2, 0.2), 0.2, 1.0)
    expert_gain = jnp.clip(1.0 + 0.18 * jax.random.normal(key_of[9], (D,), jnp.float32), 0.1, 1.9)
    expert_gate = normal_values(key_of[10], (EXPERTS, D, FF_E), D ** -0.5, 0.125, ((0, 16), (2, 16)))
    expert_up = normal_values(key_of[11], (EXPERTS, D, FF_E), D ** -0.5, 0.125, ((0, 16), (2, 16)))
    expert_down = normal_values(key_of[12], (EXPERTS, FF_E, D), FF_E ** -0.5, 0.0625, ((0, 16), (1, 16)))
    return dict(conv_value=conv_value, conv_gate=conv_gate, conv_taps=conv_taps, norm_gain=norm_gain, norm_bias=norm_bias, out_weight=out_weight, stream=stream, routes=routes, route_weights=route_weights, expert_gain=expert_gain, expert_gate=expert_gate, expert_up=expert_up, expert_down=expert_down)


epsilon = 1e-06

def reference(conv_value, conv_gate, conv_taps, norm_gain, norm_bias, out_weight, stream, routes, route_weights, expert_gain, expert_gate, expert_up, expert_down):
    f32 = jnp.float32
    gated_input = (conv_value.astype(f32) * jax.nn.sigmoid(conv_gate.astype(f32))).astype(jnp.bfloat16)
    padded = jnp.pad(gated_input.astype(f32), ((0, 0), (KERNEL - 1, 0)))
    conv_sum = jnp.zeros((CONV_CH, TOKENS), f32)
    for offset in range(KERNEL):
        conv_sum = conv_sum + conv_taps[:, offset:offset + 1] * padded[:, offset:offset + TOKENS]
    conv_float = lax.optimization_barrier(conv_sum.astype(jnp.bfloat16)).astype(f32)
    center = lax.optimization_barrier(jnp.mean(conv_float, axis=0, keepdims=True))
    spread = lax.optimization_barrier(jnp.mean((conv_float - center) ** 2, axis=0, keepdims=True))
    scaled = (conv_float - center) * lax.rsqrt(spread + epsilon) * norm_gain[:, None] + norm_bias[:, None]
    activated = jax.nn.silu(scaled).astype(jnp.bfloat16)
    projected = lax.dot_general(activated, out_weight, (((0,), (0,)), ((), ())), preferred_element_type=f32)
    residual = (stream.astype(f32) + projected).astype(jnp.bfloat16)
    res_float = residual.astype(f32)
    normed = (res_float * lax.rsqrt(lax.optimization_barrier(jnp.mean(res_float * res_float, axis=1, keepdims=True)) + epsilon) * expert_gain).astype(jnp.bfloat16)
    blocks = TOKENS // TOK_DEV
    flat_ids = routes.reshape(blocks, TOK_DEV * TOP)
    onehot = (flat_ids[:, :, None] == jnp.arange(EXPERTS, dtype=jnp.int32)[None, None, :]).astype(jnp.int32)
    before = jnp.cumsum(onehot, axis=1) - onehot
    rank = lax.optimization_barrier(jnp.sum(before * onehot, axis=2))
    row_slot = jnp.arange(blocks, dtype=jnp.int32)[:, None] * CAP + rank
    token_of = (jnp.arange(blocks, dtype=jnp.int32)[:, None] * TOK_DEV + jnp.arange(TOK_DEV * TOP, dtype=jnp.int32)[None, :] // TOP).astype(jnp.int32)
    table = jnp.full((EXPERTS, blocks * CAP), TOKENS, jnp.int32).at[flat_ids, row_slot].set(token_of)
    weight_table = jnp.zeros((EXPERTS, blocks * CAP), f32).at[flat_ids, row_slot].set(route_weights.reshape(blocks, TOK_DEV * TOP))
    padded_rows = jnp.concatenate([normed, jnp.zeros((1, D), jnp.bfloat16)], axis=0)
    width_block = FF_E // N_TP

    def per_expert(total, inputs):
        index, weights, gate_w, up_w, down_w = inputs
        rows = padded_rows[index]
        gate_val = jnp.dot(rows, gate_w, preferred_element_type=f32)
        up_val = jnp.dot(rows, up_w, preferred_element_type=f32)
        hidden = (jax.nn.silu(gate_val) * up_val).astype(jnp.bfloat16)
        result = jnp.zeros((rows.shape[0], D), f32)
        for block in range(N_TP):
            part_sum = jnp.dot(hidden[:, block * width_block:(block + 1) * width_block], down_w[block * width_block:(block + 1) * width_block], preferred_element_type=f32)
            result = result + lax.optimization_barrier(part_sum.astype(jnp.bfloat16)).astype(f32)
        result = lax.optimization_barrier(result.astype(jnp.bfloat16)).astype(f32)
        return (total.at[index].add(weights[:, None] * result), None)
    start = jnp.zeros((TOKENS + 1, D), f32)
    total, unused = lax.scan(per_expert, start, (table, weight_table, expert_gate, expert_up, expert_down))
    return (res_float + total[:TOKENS]).astype(jnp.bfloat16)
```

```python
import functools

import jax
import jax.numpy as jnp
from jax import lax
from jax.experimental import pallas as pl
from jax.experimental.pallas import tpu as pltpu
from jax.sharding import PartitionSpec as P

epsilon = 1e-06
BF16 = jnp.bfloat16
F32 = jnp.float32
MESH = pl.DeviceIdType.MESH


def moe_kernel(
    nsp,
    nz,
    normed_ref,
    resid_ref,
    routes_ref,
    routes_t_ref,
    weights_ref,
    gate_ref,
    up_ref,
    down_ref,
    out_ref,
    gate_w,
    up_w,
    down_w,
    hidden,
    sent,
    x,
    y,
    from_left,
    from_right,
    final,
    returned,
    own_sem,
    mate_send,
    mate_recv,
    disp_send,
    disp_recv,
    ag_send,
    ag_recv,
    rs_send,
    rs_recv,
    ret_send,
    ret_recv,
):
    s = lax.axis_index("sp")
    t = lax.axis_index("tp")
    z = lax.div(t, 2)
    c = lax.rem(t, 2)
    far = nz // 2
    hs = nsp // 2
    right = lax.rem(z + 1, nz) * 2 + c
    left = lax.rem(z + nz - 1, nz) * 2 + c
    mate = z * 2 + 1 - c
    cap = sent.shape[1]
    width = sent.shape[2]
    tokens = normed_ref.shape[0]
    slots = nsp * cap
    shift = cap.bit_length() - 1

    def half(ref, q, h):
        return ref.at[q, pl.ds(h * hs, hs)]

    def remote(src, dst, send, recv, sp, tp):
        return pltpu.make_async_remote_copy(
            src_ref=src,
            dst_ref=dst,
            send_sem=send,
            recv_sem=recv,
            device_id={"sp": sp, "tp": tp},
            device_id_type=MESH,
        )

    pairs = ((gate_ref, gate_w), (up_ref, up_w), (down_ref, down_w))
    for i, (src, dst) in enumerate(pairs):
        pltpu.make_async_copy(src.at[0], dst.at[0], own_sem.at[i]).start()

    barrier = pltpu.get_barrier_semaphore()

    def greet(i, carry):
        pl.semaphore_signal(
            barrier,
            inc=1,
            device_id={"sp": lax.rem(s + i, nsp), "tp": t},
            device_id_type=MESH,
        )
        return carry

    lax.fori_loop(1, nsp, greet, 0)
    for other in (right, left, mate):
        pl.semaphore_signal(barrier, inc=1, device_id={"sp": s, "tp": other}, device_id_type=MESH)

    slot = lax.broadcasted_iota(jnp.int32, (slots, tokens), 0)
    expert = lax.shift_right_logical(slot, shift)
    named = (routes_t_ref[0:1, :] == expert) | (routes_t_ref[1:2, :] == expert)
    before = lax.broadcasted_iota(jnp.int32, (tokens, tokens), 0) < lax.broadcasted_iota(
        jnp.int32, (tokens, tokens), 1
    )
    rank = jnp.dot(
        jnp.where(named, 1.0, 0.0).astype(BF16),
        jnp.where(before, 1.0, 0.0).astype(BF16),
        preferred_element_type=F32,
    )
    pick = named & (rank == (slot & (cap - 1)).astype(F32))
    chosen = jnp.dot(
        jnp.where(pick, 1.0, 0.0).astype(BF16), normed_ref[...], preferred_element_type=F32
    )
    sent[...] = chosen.astype(BF16).reshape(nsp, cap, width)

    pl.semaphore_wait(barrier, nsp + 2)

    def dispatch(i):
        e = lax.rem(s + i, nsp)
        return remote(sent.at[e], x.at[0, s], disp_send.at[i], disp_recv.at[i], e, t)

    def start_dispatch(i, carry):
        dispatch(i).start()
        return carry

    lax.fori_loop(1, nsp, start_dispatch, 0)
    mine = pltpu.make_async_copy(sent.at[s], x.at[0, s], disp_send.at[0])
    mine.start()

    def to_mate(i):
        src, dst = pairs[i]
        return remote(src.at[0], dst.at[1], mate_send.at[i], mate_recv.at[i], s, mate)

    for i in range(3):
        to_mate(i).start()

    def wait_dispatch(i, carry):
        dispatch(i).wait_recv()
        return carry

    lax.fori_loop(1, nsp, wait_dispatch, 0)
    mine.wait()

    def place(way, k):
        return 0 if k == 0 else (2 * k - 1 if way == 0 or k == far else 2 * k)

    def gather(way, k, h):
        return remote(
            half(x, place(way, k), h),
            half(x, place(way, k + 1), h),
            ag_send.at[way, k, h],
            ag_recv.at[place(way, k + 1), h],
            s,
            right if way == 0 else left,
        )

    def goes(way, k, h):
        return k < far - 1 or (k == far - 1 and h == way)

    def ffn(q):
        rows = x[q].reshape(slots, width)
        for b in range(2):
            g = jnp.dot(rows, gate_w[b], preferred_element_type=F32)
            u = jnp.dot(rows, up_w[b], preferred_element_type=F32)
            hidden[b] = (jax.nn.silu(g) * u).astype(BF16)
        tile = min(512, width)

        def columns(j, carry):
            cols = pl.ds(pl.multiple_of(j * tile, tile), tile)
            acc = jnp.dot(hidden[0], down_w[0, :, cols], preferred_element_type=F32)
            acc = acc + jnp.dot(hidden[1], down_w[1, :, cols], preferred_element_type=F32)
            y[q, :, :, cols] = acc.astype(BF16).reshape(nsp, cap, tile)
            return carry

        lax.fori_loop(0, width // tile, columns, 0)

    def ffn_loop(first, last):
        def body(q, carry):
            ffn(q)
            return carry

        lax.fori_loop(first, last, body, 0)

    for h in (0, 1):
        for way in (0, 1):
            hh = h if way == 0 else 1 - h
            if goes(way, 0, hh):
                gather(way, 0, hh).start()
    for i, (src, dst) in enumerate(pairs):
        pltpu.make_async_copy(src.at[0], dst.at[0], own_sem.at[i]).wait()
    for i in range(3):
        to_mate(i).wait_recv()
    ffn_loop(0, 1)
    for k in range(1, far + 1):
        for h in (0, 1):
            for way in (0, 1):
                hh = h if way == 0 else 1 - h
                if goes(way, k - 1, hh):
                    gather(way, k - 1, hh).wait_recv()
                    if goes(way, k, hh):
                        gather(way, k, hh).start()
        ffn_loop(2 * k - 1, min(2 * k + 1, nz))

    def arm(way, r):
        k = far - r
        if k == 0 or k == far:
            return 0 if k == 0 else 2 * far - 1
        return 2 * k if way == 0 else 2 * k - 1

    landed = (from_left, from_right)

    def reduce(way, r, h):
        return remote(
            half(y, arm(way, r), h),
            half(landed[way], r, h),
            rs_send.at[way, r, h],
            rs_recv.at[way, r, h],
            s,
            right if way == 0 else left,
        )

    def moves(way, r, h):
        return r > 0 or h != way

    def add(q, buf, r, h):
        tile = min(512, width)

        def columns(j, carry):
            cols = pl.ds(pl.multiple_of(j * tile, tile), tile)
            rows = pl.ds(h * hs, hs)
            y[q, rows, :, cols] = (
                y[q, rows, :, cols].astype(F32) + buf[r, rows, :, cols].astype(F32)
            ).astype(BF16)
            return carry

        lax.fori_loop(0, width // tile, columns, 0)

    for way in (0, 1):
        reduce(way, 0, 1 - way).start()
    if far > 1:
        for way in (0, 1):
            reduce(way, 1, way).start()
    for r in range(1, far):
        for h in (0, 1):
            for way in (0, 1):
                hh = 1 - h if way == 0 else h
                if r == 1 and hh == way:
                    continue
                reduce(way, r - 1, hh).wait_recv()
                add(arm(way, r), landed[way], r - 1, hh)
                reduce(way, r, hh).start()

    def give_back(i):
        e = lax.rem(s + i, nsp)
        return remote(final.at[e], returned.at[s], ret_send.at[i], ret_recv.at[i], e, t)

    for h in (0, 1):
        rows = pl.ds(h * hs, hs)
        for way in (0, 1):
            if moves(way, far - 1, h):
                reduce(way, far - 1, h).wait_recv()
        tile = min(512, width)

        def columns(j, carry):
            cols = pl.ds(pl.multiple_of(j * tile, tile), tile)
            total = y[0, rows, :, cols].astype(F32)
            for way in (0, 1):
                if moves(way, far - 1, h):
                    total = total + landed[way][far - 1, rows, :, cols].astype(F32)
            final[rows, :, cols] = total.astype(BF16)
            return carry

        lax.fori_loop(0, width // tile, columns, 0)

    def start_back(i, carry):
        give_back(i).start()
        return carry

    lax.fori_loop(1, nsp, start_back, 0)
    kept = pltpu.make_async_copy(final.at[s], returned.at[s], ret_send.at[0])
    kept.start()

    slot = lax.broadcasted_iota(jnp.int32, (tokens, slots), 1)
    expert = lax.shift_right_logical(slot, shift)
    first = routes_ref[:, 0:1] == expert
    second = routes_ref[:, 1:2] == expert
    named = first | second
    before = lax.broadcasted_iota(jnp.int32, (tokens, tokens), 1) < lax.broadcasted_iota(
        jnp.int32, (tokens, tokens), 0
    )
    rank = jnp.dot(
        jnp.where(before, 1.0, 0.0).astype(BF16),
        jnp.where(named, 1.0, 0.0).astype(BF16),
        preferred_element_type=F32,
    )
    pick = named & (rank == (slot & (cap - 1)).astype(F32))
    share = jnp.where(
        pick,
        jnp.where(first, weights_ref[:, 0:1], 0.0) + jnp.where(second, weights_ref[:, 1:2], 0.0),
        0.0,
    )
    high = share.astype(BF16)
    low = (share - high.astype(F32)).astype(BF16)

    def wait_back(i, carry):
        give_back(i).wait_recv()
        return carry

    lax.fori_loop(1, nsp, wait_back, 0)
    kept.wait()
    back = returned[...].reshape(slots, width)
    mixed = jnp.dot(high, back, preferred_element_type=F32)
    mixed = mixed + jnp.dot(low, back, preferred_element_type=F32)
    out_ref[...] = (resid_ref[...].astype(F32) + mixed).astype(BF16)

    def drain(i, carry):
        dispatch(i).wait_send()
        give_back(i).wait_send()
        return carry

    lax.fori_loop(1, nsp, drain, 0)
    for i in range(3):
        to_mate(i).wait_send()
    for way in (0, 1):
        for k in range(far):
            for h in (0, 1):
                if goes(way, k, h):
                    gather(way, k, h).wait_send()
                if moves(way, k, h):
                    reduce(way, k, h).wait_send()


def moe(nsp, nz, normed, residual, routes, route_weights, gate, up, down):
    tokens, width = normed.shape
    hid = gate.shape[2]
    cap = 2 * tokens // nsp
    far = nz // 2
    vmem = pl.BlockSpec(memory_space=pltpu.VMEM)
    hbm = pl.BlockSpec(memory_space=pl.ANY)
    dma = pltpu.SemaphoreType.DMA
    return pl.pallas_call(
        functools.partial(moe_kernel, nsp, nz),
        out_shape=jax.ShapeDtypeStruct((tokens, width), BF16),
        in_specs=[vmem] * 5 + [hbm] * 3,
        out_specs=vmem,
        scratch_shapes=[
            pltpu.VMEM((2, width, hid), BF16),
            pltpu.VMEM((2, width, hid), BF16),
            pltpu.VMEM((2, hid, width), BF16),
            pltpu.VMEM((2, nsp * cap, hid), BF16),
            pltpu.VMEM((nsp, cap, width), BF16),
            pltpu.VMEM((nz, nsp, cap, width), BF16),
            pltpu.VMEM((nz, nsp, cap, width), BF16),
            pltpu.VMEM((far, nsp, cap, width), BF16),
            pltpu.VMEM((far, nsp, cap, width), BF16),
            pltpu.VMEM((nsp, cap, width), BF16),
            pltpu.VMEM((nsp, cap, width), BF16),
            dma((3,)),
            dma((3,)),
            dma((3,)),
            dma((nsp,)),
            dma((nsp,)),
            dma((2, far, 2)),
            dma((nz, 2)),
            dma((2, far, 2)),
            dma((2, far, 2)),
            dma((nsp,)),
            dma((nsp,)),
        ],
        compiler_params=pltpu.CompilerParams(
            collective_id=0, has_side_effects=True, vmem_limit_bytes=60 * 1024 * 1024
        ),
        name="moe",
    )(normed, residual, routes, routes.T, route_weights, gate, up, down)


def shifted(value, axis, steps):
    count = lax.axis_size(axis)
    initial, last = (max(0, -steps), min(count, count - steps))
    return lax.ppermute(value, axis, [(source, source + steps) for source in range(initial, last)])


def per_device(
    conv_value,
    conv_gate,
    conv_taps,
    norm_gain,
    norm_bias,
    out_weight,
    stream,
    routes,
    route_weights,
    expert_gain,
    expert_gate,
    expert_up,
    expert_down,
):
    f32 = jnp.float32
    local_ch = conv_value.shape[0]
    run_len = conv_value.shape[1]
    kernel_len = conv_taps.shape[1]
    gated_input = (conv_value.astype(f32) * jax.nn.sigmoid(conv_gate.astype(f32))).astype(
        jnp.bfloat16
    )
    left_rim = shifted(gated_input[:, run_len - (kernel_len - 1) :], "sp", 1)
    padded = jnp.concatenate([left_rim, gated_input], axis=1).astype(f32)
    conv_sum = jnp.zeros((local_ch, run_len), f32)
    for offset in range(kernel_len):
        conv_sum = (
            conv_sum + conv_taps[:, offset : offset + 1] * padded[:, offset : offset + run_len]
        )
    conv_out = conv_sum.astype(jnp.bfloat16)
    whole_conv = lax.all_to_all(conv_out, "tp", split_axis=1, concat_axis=0, tiled=True).astype(f32)
    center = jnp.mean(whole_conv, axis=0, keepdims=True)
    spread = jnp.mean((whole_conv - center) ** 2, axis=0, keepdims=True)
    scaled = (whole_conv - center) * lax.rsqrt(spread + epsilon) * norm_gain[:, None] + norm_bias[
        :, None
    ]
    token_major = jax.nn.silu(scaled).astype(jnp.bfloat16)
    projected = lax.dot_general(
        token_major, out_weight, (((0,), (0,)), ((), ())), preferred_element_type=f32
    )
    residual = (stream.astype(f32) + projected).astype(jnp.bfloat16)
    res_float = residual.astype(f32)
    normed = (
        res_float
        * lax.rsqrt(jnp.mean(res_float * res_float, axis=1, keepdims=True) + epsilon)
        * expert_gain
    ).astype(jnp.bfloat16)
    return moe(
        lax.axis_size("sp"),
        lax.axis_size("tp") // 2,
        normed,
        residual,
        routes,
        route_weights,
        expert_gate,
        expert_up,
        expert_down,
    )


def solution(mesh):
    return jax.shard_map(
        per_device,
        mesh=mesh,
        in_specs=(
            P("tp", "sp"),
            P("tp", "sp"),
            P("tp", None),
            P(),
            P(),
            P(),
            P(("sp", "tp"), None),
            P(("sp", "tp"), None),
            P(("sp", "tp"), None),
            P(),
            P("sp", None, "tp"),
            P("sp", None, "tp"),
            P("sp", "tp", None),
        ),
        out_specs=P(("sp", "tp"), None),
        check_vma=False,
    )
```

```python
import functools

import jax
import jax.numpy as jnp
from jax import lax
from jax.experimental import pallas as pl
from jax.experimental.pallas import tpu as pltpu
from jax.sharding import PartitionSpec as P

epsilon = 1e-06
BF16 = jnp.bfloat16
F32 = jnp.float32
MESH = pl.DeviceIdType.MESH
by_row = (((1,), (1,)), ((), ()))


def kernel(
    nsp,
    nz,
    value_ref,
    gating_ref,
    taps_ref,
    affine_ref,
    out_w_ref,
    stream_ref,
    routes_ref,
    weights_ref,
    gain_ref,
    gate_ref,
    up_ref,
    down_ref,
    out_ref,
    gated,
    spread_taps,
    edge,
    rim,
    conv_out,
    conv_in,
    act,
    out_w,
    stream,
    resid,
    gate_w,
    up_w,
    down_w,
    hidden,
    sent,
    x,
    y,
    from_left,
    from_right,
    final,
    returned,
    in_sem,
    rim_send,
    rim_recv,
    conv_send,
    conv_recv,
    own_sem,
    mate_send,
    mate_recv,
    disp_send,
    disp_recv,
    ag_send,
    ag_recv,
    rs_send,
    rs_recv,
    ret_send,
    ret_recv,
):
    s = lax.axis_index("sp")
    t = lax.axis_index("tp")
    z = lax.div(t, 2)
    c = lax.rem(t, 2)
    far = nz // 2
    hs = nsp // 2
    right = lax.rem(z + 1, nz) * 2 + c
    left = lax.rem(z + nz - 1, nz) * 2 + c
    mate = z * 2 + 1 - c
    cap = sent.shape[1]
    width = sent.shape[2]
    tokens = routes_ref.shape[1]
    slots = nsp * cap
    shift = cap.bit_length() - 1
    local_ch, run_len = value_ref.shape
    taps = taps_ref.shape[0]
    lanes = 2 * tokens
    sub = local_ch // 2
    group = act.shape[2]
    channels = 2 * group
    tile = min(512, width)

    def half(ref, q, h):
        return ref.at[q, pl.ds(h * hs, hs)]

    def remote(src, dst, send, recv, sp, tp):
        return pltpu.make_async_remote_copy(
            src_ref=src,
            dst_ref=dst,
            send_sem=send,
            recv_sem=recv,
            device_id={"sp": sp, "tp": tp},
            device_id_type=MESH,
        )

    pairs = ((gate_ref, gate_w), (up_ref, up_w), (down_ref, down_w))
    for i, (src, dst) in enumerate(pairs):
        pltpu.make_async_copy(src.at[0], dst.at[0], own_sem.at[i]).start()

    loads = [
        pltpu.make_async_copy(out_w_ref.at[:, 0], out_w.at[0], in_sem.at[0]),
        pltpu.make_async_copy(out_w_ref.at[:, 1], out_w.at[1], in_sem.at[1]),
        pltpu.make_async_copy(stream_ref, stream, in_sem.at[2]),
    ]
    for load in loads:
        load.start()

    barrier = pltpu.get_barrier_semaphore()

    def greet_sp(i, carry):
        pl.semaphore_signal(
            barrier,
            inc=1,
            device_id={"sp": lax.rem(s + i, nsp), "tp": t},
            device_id_type=MESH,
        )
        return carry

    def greet_tp(i, carry):
        pl.semaphore_signal(
            barrier,
            inc=1,
            device_id={"sp": s, "tp": lax.rem(t + i, 2 * nz)},
            device_id_type=MESH,
        )
        return carry

    lax.fori_loop(1, nsp, greet_sp, 0)
    lax.fori_loop(1, 2 * nz, greet_tp, 0)

    for p in range(nz - 1, -1, -1):
        cols = slice(p * lanes, (p + 1) * lanes)
        product = value_ref[:, cols].astype(F32) * jax.nn.sigmoid(gating_ref[:, cols].astype(F32))
        if p == nz - 1:
            edge[...] = product.astype(BF16)
        gated[p + 1] = product.astype(BF16).astype(F32)
    by_channel = taps_ref[...].T
    for j in range(taps):
        spread_taps[j] = jnp.broadcast_to(by_channel[:, j : j + 1], (local_ch, lanes))

    pl.semaphore_wait(barrier, nsp + 2 * nz - 2)

    def to_next():
        return remote(edge, rim, rim_send.at[0], rim_recv.at[0], lax.rem(s + 1, nsp), t)

    @pl.when(s < nsp - 1)
    def _():
        to_next().start()

    def to_owner(p, core):
        return remote(
            conv_out.at[p, core], conv_in.at[t], conv_send.at[p, core], conv_recv.at[t], s, 2 * p + core
        )

    def stays(p, core):
        return pltpu.make_async_copy(conv_out.at[p, core], conv_in.at[t], conv_recv.at[t])

    lane = lax.broadcasted_iota(jnp.int32, (local_ch, lanes), 1)
    low_lanes = lax.broadcasted_iota(jnp.int32, (sub, lanes), 1) < tokens

    def conv_tile(i, carry):
        p = nz - 1 - i

        @pl.when(p == 0)
        def _():
            @pl.when(s > 0)
            def _():
                to_next().wait_recv()
                gated[0] = rim[...].astype(F32)

            @pl.when(s == 0)
            def _():
                gated[0] = jnp.zeros((local_ch, lanes), F32)

        here, before = gated[p + 1], gated[p]
        total = spread_taps[taps - 1] * here
        for d in range(1, taps):
            window = pltpu.roll(jnp.where(lane >= lanes - d, before, here), d, 1)
            total = total + spread_taps[taps - 1 - d] * window
        top, bottom = total[:sub], total[sub:]
        conv_out[p, 0] = jnp.where(low_lanes, top, pltpu.roll(bottom, tokens, 1)).astype(BF16)
        conv_out[p, 1] = jnp.where(low_lanes, pltpu.roll(top, tokens, 1), bottom).astype(BF16)
        for core in (0, 1):

            @pl.when(2 * p + core != t)
            def _():
                to_owner(p, core).start()

            @pl.when(2 * p + core == t)
            def _():
                stays(p, core).start()

        return carry

    lax.fori_loop(0, nz, conv_tile, 0)

    def to_mate(i):
        src, dst = pairs[i]
        return remote(src.at[0], dst.at[1], mate_send.at[i], mate_recv.at[i], s, mate)

    for i in range(3):
        to_mate(i).start()

    def wait_conv(i, carry):
        @pl.when(i != t)
        def _():
            remote(
                conv_out.at[0, 0], conv_in.at[i], conv_send.at[0, 0], conv_recv.at[i], s, i
            ).wait_recv()

        @pl.when(i == t)
        def _():
            stays(z, 0).wait()

        return carry

    lax.fori_loop(0, 2 * nz, wait_conv, 0)

    def over_channels(value):
        part = jnp.sum(value, axis=0, keepdims=True)
        return (part + pltpu.roll(part, tokens, 1)) * (1.0 / channels)

    whole = conv_in[...].reshape(group, lanes).astype(F32)
    deviation = whole - over_channels(whole)
    spread = over_channels(deviation * deviation)
    scaled = (deviation * lax.rsqrt(spread + epsilon)).T
    for h in (0, 1):
        part = scaled[h * tokens : (h + 1) * tokens]
        act[h] = jax.nn.silu(part * affine_ref[h : h + 1, :] + affine_ref[2 + h : 3 + h, :]).astype(
            BF16
        )
    for load in loads:
        load.wait()

    def project(j, squares):
        cols = pl.ds(pl.multiple_of(j * tile, tile), tile)
        acc = stream[:, cols].astype(F32)
        for h in (0, 1):
            acc = acc + jnp.dot(
                act[h], out_w[h, :, :, cols].reshape(group, tile), preferred_element_type=F32
            )
        rounded = acc.astype(BF16)
        resid[:, cols] = rounded
        wide = rounded.astype(F32)
        return squares + jnp.sum(wide * wide, axis=1, keepdims=True)

    squares = lax.fori_loop(0, width // tile, project, jnp.zeros((tokens, 1), F32))
    scale = lax.rsqrt(squares * (1.0 / width) + epsilon)

    slot = lax.broadcasted_iota(jnp.int32, (slots, tokens), 0)
    expert = lax.shift_right_logical(slot, shift)
    first = routes_ref[0:1, :] == expert
    second = routes_ref[1:2, :] == expert
    named = first | second
    before = lax.broadcasted_iota(jnp.int32, (tokens, tokens), 0) < lax.broadcasted_iota(
        jnp.int32, (tokens, tokens), 1
    )
    rank = jnp.dot(
        jnp.where(named, 1.0, 0.0).astype(BF16),
        jnp.where(before, 1.0, 0.0).astype(BF16),
        preferred_element_type=F32,
    )
    pick = named & (rank == (slot & (cap - 1)).astype(F32))
    chooser = jnp.where(pick, 1.0, 0.0).astype(BF16)

    def fill(j, carry):
        cols = pl.ds(pl.multiple_of(j * tile, tile), tile)
        normed = (resid[:, cols].astype(F32) * scale * gain_ref[:, cols]).astype(BF16)
        chosen = jnp.dot(chooser, normed, preferred_element_type=F32)
        sent[:, :, cols] = chosen.astype(BF16).reshape(nsp, cap, tile)
        return carry

    lax.fori_loop(0, width // tile, fill, 0)

    def dispatch(i):
        e = lax.rem(s + i, nsp)
        return remote(sent.at[e], x.at[0, s], disp_send.at[i], disp_recv.at[i], e, t)

    def start_dispatch(i, carry):
        dispatch(i).start()
        return carry

    lax.fori_loop(1, nsp, start_dispatch, 0)
    mine = pltpu.make_async_copy(sent.at[s], x.at[0, s], disp_send.at[0])
    mine.start()

    def wait_dispatch(i, carry):
        dispatch(i).wait_recv()
        return carry

    lax.fori_loop(1, nsp, wait_dispatch, 0)
    mine.wait()

    def place(way, k):
        return 0 if k == 0 else (2 * k - 1 if way == 0 or k == far else 2 * k)

    def gather(way, k, h):
        return remote(
            half(x, place(way, k), h),
            half(x, place(way, k + 1), h),
            ag_send.at[way, k, h],
            ag_recv.at[place(way, k + 1), h],
            s,
            right if way == 0 else left,
        )

    def goes(way, k, h):
        return k < far - 1 or (k == far - 1 and h == way)

    def ffn(q):
        rows = x[q].reshape(slots, width)
        for b in range(2):
            g = lax.dot_general(rows, gate_w[b], by_row, preferred_element_type=F32)
            u = lax.dot_general(rows, up_w[b], by_row, preferred_element_type=F32)
            hidden[b] = (jax.nn.silu(g) * u).astype(BF16)

        def columns(j, carry):
            cols = pl.ds(pl.multiple_of(j * tile, tile), tile)
            acc = jnp.dot(hidden[0], down_w[0, :, cols], preferred_element_type=F32)
            acc = acc + jnp.dot(hidden[1], down_w[1, :, cols], preferred_element_type=F32)
            y[q, :, :, cols] = acc.astype(BF16).reshape(nsp, cap, tile)
            return carry

        lax.fori_loop(0, width // tile, columns, 0)

    def ffn_loop(first, last):
        def body(q, carry):
            ffn(q)
            return carry

        lax.fori_loop(first, last, body, 0)

    for h in (0, 1):
        for way in (0, 1):
            hh = h if way == 0 else 1 - h
            if goes(way, 0, hh):
                gather(way, 0, hh).start()
    for i, (src, dst) in enumerate(pairs):
        pltpu.make_async_copy(src.at[0], dst.at[0], own_sem.at[i]).wait()
    for i in range(3):
        to_mate(i).wait_recv()
    ffn_loop(0, 1)
    for k in range(1, far + 1):
        for h in (0, 1):
            for way in (0, 1):
                hh = h if way == 0 else 1 - h
                if goes(way, k - 1, hh):
                    gather(way, k - 1, hh).wait_recv()
                    if goes(way, k, hh):
                        gather(way, k, hh).start()
        ffn_loop(2 * k - 1, min(2 * k + 1, nz))

    def arm(way, r):
        k = far - r
        if k == 0 or k == far:
            return 0 if k == 0 else 2 * far - 1
        return 2 * k if way == 0 else 2 * k - 1

    landed = (from_left, from_right)

    def reduce(way, r, h):
        return remote(
            half(y, arm(way, r), h),
            half(landed[way], r, h),
            rs_send.at[way, r, h],
            rs_recv.at[way, r, h],
            s,
            right if way == 0 else left,
        )

    def moves(way, r, h):
        return r > 0 or h != way

    def add(q, buf, r, h):

        def columns(j, carry):
            cols = pl.ds(pl.multiple_of(j * tile, tile), tile)
            rows = pl.ds(h * hs, hs)
            y[q, rows, :, cols] = (
                y[q, rows, :, cols].astype(F32) + buf[r, rows, :, cols].astype(F32)
            ).astype(BF16)
            return carry

        lax.fori_loop(0, width // tile, columns, 0)

    for way in (0, 1):
        reduce(way, 0, 1 - way).start()
    if far > 1:
        for way in (0, 1):
            reduce(way, 1, way).start()
    for r in range(1, far):
        for h in (0, 1):
            for way in (0, 1):
                hh = 1 - h if way == 0 else h
                if r == 1 and hh == way:
                    continue
                reduce(way, r - 1, hh).wait_recv()
                add(arm(way, r), landed[way], r - 1, hh)
                reduce(way, r, hh).start()

    def give_back(i):
        e = lax.rem(s + i, nsp)
        return remote(final.at[e], returned.at[s], ret_send.at[i], ret_recv.at[i], e, t)

    for h in (0, 1):
        rows = pl.ds(h * hs, hs)
        for way in (0, 1):
            if moves(way, far - 1, h):
                reduce(way, far - 1, h).wait_recv()

        def columns(j, carry):
            cols = pl.ds(pl.multiple_of(j * tile, tile), tile)
            total = y[0, rows, :, cols].astype(F32)
            for way in (0, 1):
                if moves(way, far - 1, h):
                    total = total + landed[way][far - 1, rows, :, cols].astype(F32)
            final[rows, :, cols] = total.astype(BF16)
            return carry

        lax.fori_loop(0, width // tile, columns, 0)

    def start_back(i, carry):
        give_back(i).start()
        return carry

    lax.fori_loop(1, nsp, start_back, 0)
    kept = pltpu.make_async_copy(final.at[s], returned.at[s], ret_send.at[0])
    kept.start()

    share = jnp.where(
        pick,
        jnp.where(first, weights_ref[0:1, :], 0.0) + jnp.where(second, weights_ref[1:2, :], 0.0),
        0.0,
    ).T
    high = share.astype(BF16)
    low = (share - high.astype(F32)).astype(BF16)

    def wait_back(i, carry):
        give_back(i).wait_recv()
        return carry

    lax.fori_loop(1, nsp, wait_back, 0)
    kept.wait()
    back = returned[...].reshape(slots, width)
    mixed = jnp.dot(high, back, preferred_element_type=F32)
    mixed = mixed + jnp.dot(low, back, preferred_element_type=F32)
    out_ref[...] = (resid[...].astype(F32) + mixed).astype(BF16)

    @pl.when(s < nsp - 1)
    def _():
        to_next().wait_send()

    def drain_conv(p, carry):
        for core in (0, 1):

            @pl.when(2 * p + core != t)
            def _():
                to_owner(p, core).wait_send()

        return carry

    lax.fori_loop(0, nz, drain_conv, 0)

    def drain(i, carry):
        dispatch(i).wait_send()
        give_back(i).wait_send()
        return carry

    lax.fori_loop(1, nsp, drain, 0)
    for i in range(3):
        to_mate(i).wait_send()
    for way in (0, 1):
        for k in range(far):
            for h in (0, 1):
                if goes(way, k, h):
                    gather(way, k, h).wait_send()
                if moves(way, k, h):
                    reduce(way, k, h).wait_send()


def per_device(
    conv_value,
    conv_gate,
    conv_taps,
    norm_gain,
    norm_bias,
    out_weight,
    stream,
    routes,
    route_weights,
    expert_gain,
    expert_gate,
    expert_up,
    expert_down,
):
    nsp, ntp = lax.axis_size("sp"), lax.axis_size("tp")
    nz = ntp // 2
    tokens, width = stream.shape
    local_ch, taps = conv_taps.shape
    sub = local_ch // 2
    hid = expert_gate.shape[2]
    cap = 2 * tokens // nsp
    far = nz // 2
    lanes = 2 * tokens
    group = ntp * sub
    affine = jnp.stack([norm_gain, norm_bias]).reshape(2, ntp, 2, sub)
    affine = affine.transpose(0, 2, 1, 3).reshape(4, group)
    vmem = pl.BlockSpec(memory_space=pltpu.VMEM)
    hbm = pl.BlockSpec(memory_space=pl.ANY)
    dma = pltpu.SemaphoreType.DMA
    return pl.pallas_call(
        functools.partial(kernel, nsp, nz),
        out_shape=jax.ShapeDtypeStruct((tokens, width), BF16),
        in_specs=[vmem] * 4 + [hbm] * 2 + [vmem] * 3 + [hbm] * 3,
        out_specs=vmem,
        scratch_shapes=[
            pltpu.VMEM((nz + 1, local_ch, lanes), F32),
            pltpu.VMEM((taps, local_ch, lanes), F32),
            pltpu.VMEM((local_ch, lanes), BF16),
            pltpu.VMEM((local_ch, lanes), BF16),
            pltpu.VMEM((nz, 2, sub, lanes), BF16),
            pltpu.VMEM((ntp, sub, lanes), BF16),
            pltpu.VMEM((2, tokens, group), BF16),
            pltpu.VMEM((2, ntp, sub, width), BF16),
            pltpu.VMEM((tokens, width), BF16),
            pltpu.VMEM((tokens, width), BF16),
            pltpu.VMEM((2, hid, width), BF16),
            pltpu.VMEM((2, hid, width), BF16),
            pltpu.VMEM((2, hid, width), BF16),
            pltpu.VMEM((2, nsp * cap, hid), BF16),
            pltpu.VMEM((nsp, cap, width), BF16),
            pltpu.VMEM((nz, nsp, cap, width), BF16),
            pltpu.VMEM((nz, nsp, cap, width), BF16),
            pltpu.VMEM((far, nsp, cap, width), BF16),
            pltpu.VMEM((far, nsp, cap, width), BF16),
            pltpu.VMEM((nsp, cap, width), BF16),
            pltpu.VMEM((nsp, cap, width), BF16),
            dma((3,)),
            dma((1,)),
            dma((1,)),
            dma((nz, 2)),
            dma((ntp,)),
            dma((3,)),
            dma((3,)),
            dma((3,)),
            dma((nsp,)),
            dma((nsp,)),
            dma((2, far, 2)),
            dma((nz, 2)),
            dma((2, far, 2)),
            dma((2, far, 2)),
            dma((nsp,)),
            dma((nsp,)),
        ],
        compiler_params=pltpu.CompilerParams(
            collective_id=0, has_side_effects=True, vmem_limit_bytes=60 * 1024 * 1024
        ),
        name="block",
    )(
        conv_value,
        conv_gate,
        conv_taps.T,
        affine,
        out_weight.reshape(ntp, 2, sub, width),
        stream,
        routes.T,
        route_weights.T,
        expert_gain[None, :],
        expert_gate.swapaxes(1, 2),
        expert_up.swapaxes(1, 2),
        expert_down,
    )


def solution(mesh):
    return jax.shard_map(
        per_device,
        mesh=mesh,
        in_specs=(
            P("tp", "sp"),
            P("tp", "sp"),
            P("tp", None),
            P(),
            P(),
            P(),
            P(("sp", "tp"), None),
            P(("sp", "tp"), None),
            P(("sp", "tp"), None),
            P(),
            P("sp", None, "tp"),
            P("sp", None, "tp"),
            P("sp", "tp", None),
        ),
        out_specs=P(("sp", "tp"), None),
        check_vma=False,
    )
```

```python
import functools

import jax
import jax.numpy as jnp
from jax import lax
from jax.experimental import pallas as pl
from jax.experimental.pallas import tpu as pltpu
from jax.sharding import PartitionSpec as P

epsilon = 1e-06
BF16 = jnp.bfloat16
F32 = jnp.float32
MESH = pl.DeviceIdType.MESH
by_row = (((1,), (1,)), ((), ()))


def kernel(
    nsp,
    nz,
    early,
    value_ref,
    gating_ref,
    taps_ref,
    norm_gain_ref,
    norm_bias_ref,
    out_w_ref,
    stream_ref,
    routes_ref,
    weights_ref,
    gain_ref,
    gate_ref,
    up_ref,
    down_ref,
    out_ref,
    gated,
    spread_taps,
    edge,
    rim,
    conv_out,
    conv_in,
    act,
    out_w,
    stream,
    resid,
    gate_w,
    up_w,
    down_w,
    hidden,
    info,
    tokens_at,
    sent,
    x,
    y,
    back_at,
    sums,
    from_left,
    from_right,
    sums_left,
    sums_right,
    final,
    returned,
    in_sem,
    rim_send,
    rim_recv,
    conv_send,
    conv_recv,
    own_sem,
    mate_send,
    mate_recv,
    info_send,
    info_recv,
    disp_send,
    disp_recv,
    plane_send,
    plane_recv,
    tok_send,
    tok_recv,
    ag_send,
    ag_recv,
    rs_send,
    rs_recv,
    sum_send,
    sum_recv,
    back_send,
    back_recv,
    ret_send,
    ret_recv,
):
    s = lax.axis_index("sp")
    t = lax.axis_index("tp")
    z = lax.div(t, 2)
    c = lax.rem(t, 2)
    far = nz // 2
    hs = nsp // 2
    right = lax.rem(z + 1, nz) * 2 + c
    left = lax.rem(z + nz - 1, nz) * 2 + c
    mate = z * 2 + 1 - c
    cap = sent.shape[2]
    width = sent.shape[3]
    tokens = routes_ref.shape[1]
    slots = nsp * cap
    shift = cap.bit_length() - 1
    local_ch, run_len = value_ref.shape
    taps = taps_ref.shape[0]
    lanes = 2 * tokens
    sub = local_ch // 2
    group = act.shape[2]
    channels = 2 * group
    tile = min(512, early)
    ht = tokens // 2
    late = pl.ds(early, width - early)
    ahead = pl.ds(0, early)

    def half(ref, q, h):
        return ref.at[q, pl.ds(h * hs, hs), :, late]

    def column_loop(first, last, body):
        def step(j, carry):
            body(pl.ds(pl.multiple_of(j * tile, tile), tile))
            return carry

        lax.fori_loop(first // tile, last // tile, step, 0)

    def remote(src, dst, send, recv, sp, tp):
        return pltpu.make_async_remote_copy(
            src_ref=src,
            dst_ref=dst,
            send_sem=send,
            recv_sem=recv,
            device_id={"sp": sp, "tp": tp},
            device_id_type=MESH,
        )

    pairs = ((gate_ref, gate_w), (up_ref, up_w), (down_ref, down_w))
    for i, (src, dst) in enumerate(pairs):
        pltpu.make_async_copy(src.at[0], dst.at[0], own_sem.at[i]).start()

    loads = [
        pltpu.make_async_copy(out_w_ref.at[:, 0], out_w.at[0], in_sem.at[0]),
        pltpu.make_async_copy(out_w_ref.at[:, 1], out_w.at[1], in_sem.at[1]),
        pltpu.make_async_copy(stream_ref, stream, in_sem.at[2]),
    ]
    for load in loads:
        load.start()

    barrier = pltpu.get_barrier_semaphore()

    def greet_sp(i, carry):
        pl.semaphore_signal(
            barrier,
            inc=1,
            device_id={"sp": lax.rem(s + i, nsp), "tp": t},
            device_id_type=MESH,
        )
        return carry

    def greet_tp(i, carry):
        pl.semaphore_signal(
            barrier,
            inc=1,
            device_id={"sp": s, "tp": lax.rem(t + i, 2 * nz)},
            device_id_type=MESH,
        )
        return carry

    lax.fori_loop(1, nsp, greet_sp, 0)
    lax.fori_loop(1, 2 * nz, greet_tp, 0)

    for p in range(nz - 1, -1, -1):
        cols = slice(p * lanes, (p + 1) * lanes)
        product = value_ref[:, cols].astype(F32) * jax.nn.sigmoid(gating_ref[:, cols].astype(F32))
        if p == nz - 1:
            edge[...] = product.astype(BF16)
        gated[p + 1] = product.astype(BF16).astype(F32)
    by_channel = taps_ref[...].T
    for j in range(taps):
        spread_taps[j] = jnp.broadcast_to(by_channel[:, j : j + 1], (local_ch, lanes))

    slot = lax.broadcasted_iota(jnp.int32, (slots, tokens), 0)
    expert = lax.shift_right_logical(slot, shift)
    first = routes_ref[0:1, :] == expert
    second = routes_ref[1:2, :] == expert
    named = first | second
    before = lax.broadcasted_iota(jnp.int32, (tokens, tokens), 0) < lax.broadcasted_iota(
        jnp.int32, (tokens, tokens), 1
    )
    rank = jnp.dot(
        jnp.where(named, 1.0, 0.0).astype(BF16),
        jnp.where(before, 1.0, 0.0).astype(BF16),
        preferred_element_type=F32,
    )
    pick = named & (rank == (slot & (cap - 1)).astype(F32))
    number = slot.astype(F32)
    info[0] = jnp.zeros((8, lanes), F32)
    for i, hit in enumerate((first, second)):
        info[0, i : i + 1, :tokens] = jnp.sum(
            jnp.where(hit & pick, number, 0.0), axis=0, keepdims=True
        )
        info[0, 2 + i : 3 + i, :tokens] = weights_ref[i : i + 1, :]

    def regroup(ref, h):
        return jnp.concatenate(
            [ref[:, pl.ds((2 * i + h) * sub, sub)] for i in range(2 * nz)], axis=1
        )

    affine = [(regroup(norm_gain_ref, h), regroup(norm_bias_ref, h)) for h in (0, 1)]

    pl.semaphore_wait(barrier, nsp + 2 * nz - 2)

    def to_next():
        return remote(edge, rim, rim_send.at[0], rim_recv.at[0], lax.rem(s + 1, nsp), t)

    @pl.when(s < nsp - 1)
    def _():
        to_next().start()

    def tell(i):
        q = jnp.where(i <= far, 2 * i - 1, 2 * (nz - i))
        return remote(
            info.at[0], info.at[q], info_send.at[i], info_recv.at[q], s, lax.rem(z + i, nz) * 2 + c
        )

    def start_tell(i, carry):
        tell(i).start()
        return carry

    lax.fori_loop(1, nz, start_tell, 0)

    def to_owner(p, core):
        return remote(
            conv_out.at[p, core], conv_in.at[t], conv_send.at[p, core], conv_recv.at[t], s, 2 * p + core
        )

    def stays(p, core):
        return pltpu.make_async_copy(conv_out.at[p, core], conv_in.at[t], conv_recv.at[t])

    lane = lax.broadcasted_iota(jnp.int32, (local_ch, lanes), 1)
    low_lanes = lax.broadcasted_iota(jnp.int32, (sub, lanes), 1) < tokens

    def conv_tile(i, carry):
        p = nz - 1 - i

        @pl.when(p == 0)
        def _():
            @pl.when(s > 0)
            def _():
                to_next().wait_recv()
                gated[0] = rim[...].astype(F32)

            @pl.when(s == 0)
            def _():
                gated[0] = jnp.zeros((local_ch, lanes), F32)

        here, before = gated[p + 1], gated[p]
        total = spread_taps[taps - 1] * here
        for d in range(1, taps):
            window = pltpu.roll(jnp.where(lane >= lanes - d, before, here), d, 1)
            total = total + spread_taps[taps - 1 - d] * window
        top, bottom = total[:sub], total[sub:]
        conv_out[p, 0] = jnp.where(low_lanes, top, pltpu.roll(bottom, tokens, 1)).astype(BF16)
        conv_out[p, 1] = jnp.where(low_lanes, pltpu.roll(top, tokens, 1), bottom).astype(BF16)
        for core in (0, 1):

            @pl.when(2 * p + core != t)
            def _():
                to_owner(p, core).start()

            @pl.when(2 * p + core == t)
            def _():
                stays(p, core).start()

        return carry

    lax.fori_loop(0, nz, conv_tile, 0)

    def to_mate(i):
        src, dst = pairs[i]
        return remote(src.at[0], dst.at[1], mate_send.at[i], mate_recv.at[i], s, mate)

    for i in range(3):
        to_mate(i).start()

    def wait_conv(i, carry):
        @pl.when(i != t)
        def _():
            remote(
                conv_out.at[0, 0], conv_in.at[i], conv_send.at[0, 0], conv_recv.at[i], s, i
            ).wait_recv()

        @pl.when(i == t)
        def _():
            stays(z, 0).wait()

        return carry

    lax.fori_loop(0, 2 * nz, wait_conv, 0)

    def over_channels(value):
        part = jnp.sum(value, axis=0, keepdims=True)
        return (part + pltpu.roll(part, tokens, 1)) * (1.0 / channels)

    whole = conv_in[...].reshape(group, lanes).astype(F32)
    deviation = whole - over_channels(whole)
    spread = over_channels(deviation * deviation)
    scaled = (deviation * lax.rsqrt(spread + epsilon)).T
    for h in (0, 1):
        part = scaled[h * tokens : (h + 1) * tokens]
        act[h] = jax.nn.silu(part * affine[h][0] + affine[h][1]).astype(
            BF16
        )
    for load in loads:
        load.wait()

    def project(j, squares):
        cols = pl.ds(pl.multiple_of(j * tile, tile), tile)
        acc = stream[:, cols].astype(F32)
        for h in (0, 1):
            acc = acc + jnp.dot(
                act[h], out_w[h, :, :, cols].reshape(group, tile), preferred_element_type=F32
            )
        rounded = acc.astype(BF16)
        resid[:, cols] = rounded
        wide = rounded.astype(F32)
        return squares + jnp.sum(wide * wide, axis=1, keepdims=True)

    squares = lax.fori_loop(0, width // tile, project, jnp.zeros((tokens, 1), F32))
    scale = lax.rsqrt(squares * (1.0 / width) + epsilon)

    def place(way, k):
        return 0 if k == 0 else (2 * k - 1 if way == 0 or k == far else 2 * k)

    def goes(way, k, h):
        return k < far - 1 or (k == far - 1 and h == way)

    def spread(way, k, h):
        return remote(
            tokens_at.at[place(way, k), h],
            tokens_at.at[place(way, k + 1), h],
            tok_send.at[way, k, h],
            tok_recv.at[place(way, k + 1), h],
            s,
            right if way == 0 else left,
        )

    def start_hop(copy, k):
        for h in (0, 1):
            for way in (0, 1):
                hh = h if way == 0 else 1 - h
                if goes(way, k, hh):
                    copy(way, k, hh).start()

    def pass_on(copy, k):
        for h in (0, 1):
            for way in (0, 1):
                hh = h if way == 0 else 1 - h
                if goes(way, k - 1, hh):
                    copy(way, k - 1, hh).wait_recv()
                    if goes(way, k, hh):
                        copy(way, k, hh).start()

    def normalize(cols):
        return (resid[:, cols].astype(F32) * scale * gain_ref[:, cols]).astype(BF16)

    def set_tokens(cols):
        tokens_at[0, :, :, cols] = normalize(cols).reshape(2, ht, tile)

    column_loop(0, early, set_tokens)
    start_hop(spread, 0)

    slot_of = lax.broadcasted_iota(jnp.int32, (slots, tokens), 0).astype(F32)

    def hits(q, i):
        return slot_of == info[q, i : i + 1, :tokens]

    def chooser(q):
        return jnp.where(hits(q, 0) | hits(q, 1), 1.0, 0.0).astype(BF16)

    def weigher(q):
        share = jnp.where(hits(q, 0), info[q, 2:3, :tokens], 0.0) + jnp.where(
            hits(q, 1), info[q, 3:4, :tokens], 0.0
        )
        share = share.T
        high = share.astype(BF16)
        return high, (share - high.astype(F32)).astype(BF16)

    def choose(q, rows, cols, pick):
        chosen = jnp.dot(pick, rows, preferred_element_type=F32)
        sent[q, :, :, cols] = chosen.astype(BF16).reshape(nsp, cap, tile)

    def over_plane(src, dst, q, cols, send, recv):
        def copy(i):
            e = lax.rem(s + i, nsp)
            return remote(src.at[q, e, :, cols], dst.at[q, s, :, cols], send, recv, e, t)

        def begin(i, carry):
            copy(i).start()
            return carry

        lax.fori_loop(1, nsp, begin, 0)
        pltpu.make_async_copy(src.at[q, s, :, cols], dst.at[q, s, :, cols], recv).start()

    def all_in(dst, q, cols, recv):
        pltpu.make_async_copy(dst.at[q, :, :, cols], dst.at[q, :, :, cols], recv).wait()

    def all_out(src, q, cols, send):
        block = src.at[q, pl.ds(0, nsp - 1), :, cols]
        pltpu.make_async_copy(block, block, send).wait()

    own_pick = chooser(0)
    column_loop(early, width, lambda cols: choose(0, normalize(cols), cols, own_pick))
    over_plane(sent, x, 0, late, disp_send.at[0], disp_recv.at[0])
    column_loop(
        0, early, lambda cols: choose(0, tokens_at[0, :, :, cols].reshape(tokens, tile), cols, own_pick)
    )
    over_plane(sent, x, 0, ahead, plane_send.at[0], plane_recv.at[0])

    def tell_in(q):
        pltpu.make_async_copy(info.at[q], info.at[q], info_recv.at[q]).wait()

    def select(q):
        tell_in(q)
        pick = chooser(q)
        column_loop(
            0, early, lambda cols: choose(q, tokens_at[q, :, :, cols].reshape(tokens, tile), cols, pick)
        )
        over_plane(sent, x, q, ahead, plane_send.at[q], plane_recv.at[q])

    def q_loop(first, last, f):
        def body(q, carry):
            f(q)
            return carry

        lax.fori_loop(first, last, body, 0)

    pass_on(spread, 1)
    q_loop(1, min(3, nz), select)
    all_in(x, 0, late, disp_recv.at[0])

    def gather(way, k, h):
        return remote(
            half(x, place(way, k), h),
            half(x, place(way, k + 1), h),
            ag_send.at[way, k, h],
            ag_recv.at[place(way, k + 1), h],
            s,
            right if way == 0 else left,
        )

    def ffn(q):
        rows = x[q].reshape(slots, width)
        for b in range(2):
            g = lax.dot_general(rows, gate_w[b], by_row, preferred_element_type=F32)
            u = lax.dot_general(rows, up_w[b], by_row, preferred_element_type=F32)
            hidden[b] = (jax.nn.silu(g) * u).astype(BF16)

        def columns(j, carry):
            cols = pl.ds(pl.multiple_of(j * tile, tile), tile)
            acc = jnp.dot(hidden[0], down_w[0, :, cols], preferred_element_type=F32)
            acc = acc + jnp.dot(hidden[1], down_w[1, :, cols], preferred_element_type=F32)
            y[q, :, :, cols] = acc.astype(BF16).reshape(nsp, cap, tile)
            return carry

        lax.fori_loop(0, width // tile, columns, 0)

    def experts(q):
        all_in(x, q, ahead, plane_recv.at[q])
        ffn(q)
        over_plane(y, back_at, q, ahead, back_send.at[q], back_recv.at[q])

    start_hop(gather, 0)
    for k in range(2, far + 1):
        pass_on(spread, k)
        q_loop(2 * k - 1, min(2 * k + 1, nz), select)
    for i, (src, dst) in enumerate(pairs):
        pltpu.make_async_copy(src.at[0], dst.at[0], own_sem.at[i]).wait()
    for i in range(3):
        to_mate(i).wait_recv()
    q_loop(0, 1, experts)
    for k in range(1, far + 1):
        pass_on(gather, k)
        q_loop(2 * k - 1, min(2 * k + 1, nz), experts)

    def arm(way, r):
        k = far - r
        if k == 0 or k == far:
            return 0 if k == 0 else 2 * far - 1
        return 2 * k if way == 0 else 2 * k - 1

    landed = (from_left, from_right)

    def reduce(way, r, h):
        return remote(
            half(y, arm(way, r), h),
            half(landed[way], r, h),
            rs_send.at[way, r, h],
            rs_recv.at[way, r, h],
            s,
            right if way == 0 else left,
        )

    def moves(way, r, h):
        return r > 0 or h != way

    def add(q, buf, r, h):
        rows = pl.ds(h * hs, hs)

        def body(cols):
            y[q, rows, :, cols] = (
                y[q, rows, :, cols].astype(F32) + buf[r, rows, :, cols].astype(F32)
            ).astype(BF16)

        column_loop(early, width, body)

    sums_landed = (sums_left, sums_right)

    def reduce_sums(way, r, h):
        return remote(
            sums.at[arm(way, r), h],
            sums_landed[way].at[r, h],
            sum_send.at[way, r, h],
            sum_recv.at[way, r, h],
            s,
            right if way == 0 else left,
        )

    def add_sums(q, buf, r, h):
        sums[q, h] = (sums[q, h].astype(F32) + buf[r, h].astype(F32)).astype(BF16)

    def combine(q):
        all_in(back_at, q, ahead, back_recv.at[q])
        high, low = weigher(q)

        def body(cols):
            rows = back_at[q, :, :, cols].reshape(slots, tile)
            mixed = jnp.dot(high, rows, preferred_element_type=F32)
            mixed = mixed + jnp.dot(low, rows, preferred_element_type=F32)
            sums[q, :, :, cols] = mixed.astype(BF16).reshape(2, ht, tile)

        column_loop(0, early, body)

    def open_arms(copy):
        for way in (0, 1):
            copy(way, 0, 1 - way).start()

    def second_halves(copy):
        if far > 1:
            for way in (0, 1):
                copy(way, 1, way).start()

    def advance(copy, plus, bufs, r):
        for h in (0, 1):
            for way in (0, 1):
                hh = 1 - h if way == 0 else h
                if r == 1 and hh == way:
                    continue
                copy(way, r - 1, hh).wait_recv()
                plus(arm(way, r), bufs[way], r - 1, hh)
                copy(way, r, hh).start()

    open_arms(reduce)
    second_halves(reduce)
    q_loop(nz - 1, nz, combine)
    open_arms(reduce_sums)
    if far > 1:
        q_loop(nz - 3, nz - 1, combine)
        second_halves(reduce_sums)
    for r in range(1, far):
        advance(reduce, add, landed, r)
        if r + 1 < far:
            q_loop(nz - 3 - 2 * r, nz - 1 - 2 * r, combine)
        advance(reduce_sums, add_sums, sums_landed, r)
    q_loop(0, 1, combine)

    for h in (0, 1):
        rows = pl.ds(h * hs, hs)
        for way in (0, 1):
            if moves(way, far - 1, h):
                reduce(way, far - 1, h).wait_recv()

        def finish(cols):
            total = y[0, rows, :, cols].astype(F32)
            for way in (0, 1):
                if moves(way, far - 1, h):
                    total = total + landed[way][far - 1, rows, :, cols].astype(F32)
            final[0, rows, :, cols] = total.astype(BF16)

        column_loop(early, width, finish)

    over_plane(final, returned, 0, late, ret_send.at[0], ret_recv.at[0])

    for h in (0, 1):
        rows = pl.ds(h * ht, ht)
        for way in (0, 1):
            if moves(way, far - 1, h):
                reduce_sums(way, far - 1, h).wait_recv()

        def finish_sums(cols):
            total = resid[rows, cols].astype(F32) + sums[0, h, :, cols].astype(F32)
            for way in (0, 1):
                if moves(way, far - 1, h):
                    total = total + sums_landed[way][far - 1, h, :, cols].astype(F32)
            out_ref[rows, cols] = total.astype(BF16)

        column_loop(0, early, finish_sums)

    high, low = weigher(0)
    all_in(returned, 0, late, ret_recv.at[0])

    def finish_late(cols):
        rows = returned[0, :, :, cols].reshape(slots, tile)
        mixed = jnp.dot(high, rows, preferred_element_type=F32)
        mixed = mixed + jnp.dot(low, rows, preferred_element_type=F32)
        out_ref[:, cols] = (resid[:, cols].astype(F32) + mixed).astype(BF16)

    column_loop(early, width, finish_late)

    @pl.when(s < nsp - 1)
    def _():
        to_next().wait_send()

    def drain_conv(p, carry):
        for core in (0, 1):

            @pl.when(2 * p + core != t)
            def _():
                to_owner(p, core).wait_send()

        return carry

    lax.fori_loop(0, nz, drain_conv, 0)

    def drain_tell(i, carry):
        tell(i).wait_send()
        return carry

    lax.fori_loop(1, nz, drain_tell, 0)
    all_out(sent, 0, late, disp_send.at[0])
    all_out(final, 0, late, ret_send.at[0])

    def drain_plane(q):
        all_out(sent, q, ahead, plane_send.at[q])
        all_out(y, q, ahead, back_send.at[q])

    q_loop(0, nz, drain_plane)
    for i in range(3):
        to_mate(i).wait_send()
    for way in (0, 1):
        for k in range(far):
            for h in (0, 1):
                if goes(way, k, h):
                    gather(way, k, h).wait_send()
                    spread(way, k, h).wait_send()
                if moves(way, k, h):
                    reduce(way, k, h).wait_send()
                    reduce_sums(way, k, h).wait_send()


def per_device(
    conv_value,
    conv_gate,
    conv_taps,
    norm_gain,
    norm_bias,
    out_weight,
    stream,
    routes,
    route_weights,
    expert_gain,
    expert_gate,
    expert_up,
    expert_down,
):
    nsp, ntp = lax.axis_size("sp"), lax.axis_size("tp")
    nz = ntp // 2
    tokens, width = stream.shape
    local_ch, taps = conv_taps.shape
    sub = local_ch // 2
    hid = expert_gate.shape[2]
    cap = 2 * tokens // nsp
    far = nz // 2
    lanes = 2 * tokens
    group = ntp * sub
    early = width // 2
    vmem = pl.BlockSpec(memory_space=pltpu.VMEM)
    hbm = pl.BlockSpec(memory_space=pl.ANY)
    dma = pltpu.SemaphoreType.DMA
    return pl.pallas_call(
        functools.partial(kernel, nsp, nz, early),
        out_shape=jax.ShapeDtypeStruct((tokens, width), BF16),
        in_specs=[vmem] * 5 + [hbm] * 2 + [vmem] * 3 + [hbm] * 3,
        out_specs=vmem,
        scratch_shapes=[
            pltpu.VMEM((nz + 1, local_ch, lanes), F32),
            pltpu.VMEM((taps, local_ch, lanes), F32),
            pltpu.VMEM((local_ch, lanes), BF16),
            pltpu.VMEM((local_ch, lanes), BF16),
            pltpu.VMEM((nz, 2, sub, lanes), BF16),
            pltpu.VMEM((ntp, sub, lanes), BF16),
            pltpu.VMEM((2, tokens, group), BF16),
            pltpu.VMEM((2, ntp, sub, width), BF16),
            pltpu.VMEM((tokens, width), BF16),
            pltpu.VMEM((tokens, width), BF16),
            pltpu.VMEM((2, hid, width), BF16),
            pltpu.VMEM((2, hid, width), BF16),
            pltpu.VMEM((2, hid, width), BF16),
            pltpu.VMEM((2, nsp * cap, hid), BF16),
            pltpu.VMEM((nz, 8, lanes), F32),
            pltpu.VMEM((nz, 2, tokens // 2, early), BF16),
            pltpu.VMEM((nz, nsp, cap, width), BF16),
            pltpu.VMEM((nz, nsp, cap, width), BF16),
            pltpu.VMEM((nz, nsp, cap, width), BF16),
            pltpu.VMEM((nz, nsp, cap, early), BF16),
            pltpu.VMEM((nz, 2, tokens // 2, early), BF16),
            pltpu.VMEM((far, nsp, cap, width), BF16),
            pltpu.VMEM((far, nsp, cap, width), BF16),
            pltpu.VMEM((far, 2, tokens // 2, early), BF16),
            pltpu.VMEM((far, 2, tokens // 2, early), BF16),
            pltpu.VMEM((1, nsp, cap, width), BF16),
            pltpu.VMEM((1, nsp, cap, width), BF16),
            dma((3,)),
            dma((1,)),
            dma((1,)),
            dma((nz, 2)),
            dma((ntp,)),
            dma((3,)),
            dma((3,)),
            dma((3,)),
            dma((nz,)),
            dma((nz,)),
            dma((1,)),
            dma((1,)),
            dma((nz,)),
            dma((nz,)),
            dma((2, far, 2)),
            dma((nz, 2)),
            dma((2, far, 2)),
            dma((nz, 2)),
            dma((2, far, 2)),
            dma((2, far, 2)),
            dma((2, far, 2)),
            dma((2, far, 2)),
            dma((nz,)),
            dma((nz,)),
            dma((1,)),
            dma((1,)),
        ],
        compiler_params=pltpu.CompilerParams(
            collective_id=0, has_side_effects=True, vmem_limit_bytes=60 * 1024 * 1024
        ),
        name="block",
    )(
        conv_value,
        conv_gate,
        conv_taps.T,
        norm_gain[None, :],
        norm_bias[None, :],
        out_weight.reshape(ntp, 2, sub, width),
        stream,
        routes.T,
        route_weights.T,
        expert_gain[None, :],
        expert_gate.swapaxes(1, 2),
        expert_up.swapaxes(1, 2),
        expert_down,
    )


def solution(mesh):
    return jax.shard_map(
        per_device,
        mesh=mesh,
        in_specs=(
            P("tp", "sp"),
            P("tp", "sp"),
            P("tp", None),
            P(),
            P(),
            P(),
            P(("sp", "tp"), None),
            P(("sp", "tp"), None),
            P(("sp", "tp"), None),
            P(),
            P("sp", None, "tp"),
            P("sp", None, "tp"),
            P("sp", "tp", None),
        ),
        out_specs=P(("sp", "tp"), None),
        check_vma=False,
    )
```

```python
import functools

import jax
import jax.numpy as jnp
from jax import lax
from jax.experimental import pallas as pl
from jax.experimental.pallas import tpu as pltpu
from jax.sharding import PartitionSpec as P

epsilon = 1e-06
BF16 = jnp.bfloat16
F32 = jnp.float32
MESH = pl.DeviceIdType.MESH
by_row = (((1,), (1,)), ((), ()))


def kernel(
    nsp,
    nz,
    early,
    value_ref,
    gating_ref,
    taps_ref,
    norm_gain_ref,
    norm_bias_ref,
    out_w_ref,
    stream_ref,
    routes_ref,
    weights_ref,
    gain_ref,
    gate_ref,
    up_ref,
    down_ref,
    out_ref,
    gated,
    spread_taps,
    edge,
    rim,
    conv_out,
    conv_in,
    act,
    out_w,
    stream,
    resid,
    gate_w,
    up_w,
    down_w,
    hidden,
    info,
    tokens_at,
    sent,
    x,
    y,
    back_at,
    sums,
    from_left,
    from_right,
    sums_left,
    sums_right,
    final,
    returned,
    in_sem,
    rim_send,
    rim_recv,
    conv_send,
    conv_recv,
    own_sem,
    mate_send,
    mate_recv,
    info_send,
    info_recv,
    disp_send,
    disp_recv,
    plane_send,
    plane_recv,
    tok_send,
    tok_recv,
    ag_send,
    ag_recv,
    rs_send,
    rs_recv,
    sum_send,
    sum_recv,
    back_send,
    back_recv,
    ret_send,
    ret_recv,
):
    s = lax.axis_index("sp")
    t = lax.axis_index("tp")
    z = lax.div(t, 2)
    c = lax.rem(t, 2)
    far = nz // 2
    hs = nsp // 2
    right = lax.rem(z + 1, nz) * 2 + c
    left = lax.rem(z + nz - 1, nz) * 2 + c
    mate = z * 2 + 1 - c
    cap = sent.shape[2]
    width = sent.shape[3]
    tokens = routes_ref.shape[1]
    slots = nsp * cap
    shift = cap.bit_length() - 1
    local_ch, run_len = value_ref.shape
    taps = taps_ref.shape[0]
    lanes = 2 * tokens
    sub = local_ch // 2
    group = act.shape[2]
    channels = 2 * group
    tile = min(512, early)
    wide = min(512, width)
    ht = tokens // 2
    late = pl.ds(early, width - early)
    ahead = pl.ds(0, early)

    def half(ref, q, h):
        return ref.at[q, pl.ds(h * hs, hs), :, late]

    def column_loop(first, last, body):
        def step(j, carry):
            body(pl.ds(pl.multiple_of(j * tile, tile), tile))
            return carry

        lax.fori_loop(first // tile, last // tile, step, 0)

    def remote(src, dst, send, recv, sp, tp):
        return pltpu.make_async_remote_copy(
            src_ref=src,
            dst_ref=dst,
            send_sem=send,
            recv_sem=recv,
            device_id={"sp": sp, "tp": tp},
            device_id_type=MESH,
        )

    loads = [
        pltpu.make_async_copy(out_w_ref.at[:, 0], out_w.at[0], in_sem.at[0]),
        pltpu.make_async_copy(out_w_ref.at[:, 1], out_w.at[1], in_sem.at[1]),
        pltpu.make_async_copy(stream_ref, stream, in_sem.at[2]),
    ]
    for load in loads:
        load.start()
    pairs = ((gate_ref, gate_w), (up_ref, up_w), (down_ref, down_w))
    for i, (src, dst) in enumerate(pairs):
        pltpu.make_async_copy(src.at[0], dst.at[0], own_sem.at[i]).start()

    barrier = pltpu.get_barrier_semaphore()

    def greet_sp(i, carry):
        pl.semaphore_signal(
            barrier,
            inc=1,
            device_id={"sp": lax.rem(s + i, nsp), "tp": t},
            device_id_type=MESH,
        )
        return carry

    def greet_tp(i, carry):
        pl.semaphore_signal(
            barrier,
            inc=1,
            device_id={"sp": s, "tp": lax.rem(t + i, 2 * nz)},
            device_id_type=MESH,
        )
        return carry

    lax.fori_loop(1, nsp, greet_sp, 0)
    lax.fori_loop(1, 2 * nz, greet_tp, 0)

    for p in range(nz - 1, -1, -1):
        cols = slice(p * lanes, (p + 1) * lanes)
        product = value_ref[:, cols].astype(F32) * jax.nn.sigmoid(gating_ref[:, cols].astype(F32))
        if p == nz - 1:
            edge[...] = product.astype(BF16)
        gated[p + 1] = product.astype(BF16).astype(F32)
    by_channel = taps_ref[...].T
    for j in range(taps):
        spread_taps[j] = jnp.broadcast_to(by_channel[:, j : j + 1], (local_ch, lanes))

    slot = lax.broadcasted_iota(jnp.int32, (slots, tokens), 0)
    expert = lax.shift_right_logical(slot, shift)
    first = routes_ref[0:1, :] == expert
    second = routes_ref[1:2, :] == expert
    named = first | second
    before = lax.broadcasted_iota(jnp.int32, (tokens, tokens), 0) < lax.broadcasted_iota(
        jnp.int32, (tokens, tokens), 1
    )
    rank = jnp.dot(
        jnp.where(named, 1.0, 0.0).astype(BF16),
        jnp.where(before, 1.0, 0.0).astype(BF16),
        preferred_element_type=F32,
    )
    pick = named & (rank == (slot & (cap - 1)).astype(F32))
    number = slot.astype(F32)
    info[0] = jnp.zeros((8, lanes), F32)
    for i, hit in enumerate((first, second)):
        info[0, i : i + 1, :tokens] = jnp.sum(
            jnp.where(hit & pick, number, 0.0), axis=0, keepdims=True
        )
        info[0, 2 + i : 3 + i, :tokens] = weights_ref[i : i + 1, :]

    def regroup(ref, h):
        return jnp.concatenate(
            [ref[:, pl.ds((2 * i + h) * sub, sub)] for i in range(2 * nz)], axis=1
        )

    affine = [(regroup(norm_gain_ref, h), regroup(norm_bias_ref, h)) for h in (0, 1)]

    pl.semaphore_wait(barrier, nsp + 2 * nz - 2)

    def to_next():
        return remote(edge, rim, rim_send.at[0], rim_recv.at[0], lax.rem(s + 1, nsp), t)

    @pl.when(s < nsp - 1)
    def _():
        to_next().start()

    def tell(i):
        q = jnp.where(i <= far, 2 * i - 1, 2 * (nz - i))
        return remote(
            info.at[0], info.at[q], info_send.at[i], info_recv.at[q], s, lax.rem(z + i, nz) * 2 + c
        )

    def start_tell(i, carry):
        tell(i).start()
        return carry

    lax.fori_loop(1, nz, start_tell, 0)

    def to_owner(p, core):
        return remote(
            conv_out.at[p, core], conv_in.at[t], conv_send.at[p, core], conv_recv.at[t], s, 2 * p + core
        )

    def stays(p, core):
        return pltpu.make_async_copy(conv_out.at[p, core], conv_in.at[t], conv_recv.at[t])

    lane = lax.broadcasted_iota(jnp.int32, (local_ch, lanes), 1)
    low_lanes = lax.broadcasted_iota(jnp.int32, (sub, lanes), 1) < tokens

    def conv_tile(i, carry):
        p = nz - 1 - i

        @pl.when(p == 0)
        def _():
            @pl.when(s > 0)
            def _():
                to_next().wait_recv()
                gated[0] = rim[...].astype(F32)

            @pl.when(s == 0)
            def _():
                gated[0] = jnp.zeros((local_ch, lanes), F32)

        here, before = gated[p + 1], gated[p]
        total = spread_taps[taps - 1] * here
        for d in range(1, taps):
            window = pltpu.roll(jnp.where(lane >= lanes - d, before, here), d, 1)
            total = total + spread_taps[taps - 1 - d] * window
        top, bottom = total[:sub], total[sub:]
        conv_out[p, 0] = jnp.where(low_lanes, top, pltpu.roll(bottom, tokens, 1)).astype(BF16)
        conv_out[p, 1] = jnp.where(low_lanes, pltpu.roll(top, tokens, 1), bottom).astype(BF16)
        for core in (0, 1):

            @pl.when(2 * p + core != t)
            def _():
                to_owner(p, core).start()

            @pl.when(2 * p + core == t)
            def _():
                stays(p, core).start()

        return carry

    lax.fori_loop(0, nz, conv_tile, 0)

    def to_mate(i):
        src, dst = pairs[i]
        return remote(src.at[0], dst.at[1], mate_send.at[i], mate_recv.at[i], s, mate)

    for i in range(3):
        to_mate(i).start()

    def wait_conv(i, carry):
        @pl.when(i != t)
        def _():
            remote(
                conv_out.at[0, 0], conv_in.at[i], conv_send.at[0, 0], conv_recv.at[i], s, i
            ).wait_recv()

        @pl.when(i == t)
        def _():
            stays(z, 0).wait()

        return carry

    lax.fori_loop(0, 2 * nz, wait_conv, 0)

    def over_channels(value):
        part = jnp.sum(value, axis=0, keepdims=True)
        return (part + pltpu.roll(part, tokens, 1)) * (1.0 / channels)

    whole = conv_in[...].reshape(group, lanes).astype(F32)
    deviation = whole - over_channels(whole)
    spread = over_channels(deviation * deviation)
    scaled = (deviation * lax.rsqrt(spread + epsilon)).T
    for h in (0, 1):
        part = scaled[h * tokens : (h + 1) * tokens]
        act[h] = jax.nn.silu(part * affine[h][0] + affine[h][1]).astype(
            BF16
        )
    for load in loads:
        load.wait()

    def project(j, squares):
        cols = pl.ds(pl.multiple_of(j * tile, tile), tile)
        acc = stream[:, cols].astype(F32)
        for h in (0, 1):
            acc = acc + jnp.dot(
                act[h], out_w[h, :, :, cols].reshape(group, tile), preferred_element_type=F32
            )
        rounded = acc.astype(BF16)
        resid[:, cols] = rounded
        wide = rounded.astype(F32)
        return squares + jnp.sum(wide * wide, axis=1, keepdims=True)

    squares = lax.fori_loop(0, width // tile, project, jnp.zeros((tokens, 1), F32))
    scale = lax.rsqrt(squares * (1.0 / width) + epsilon)

    def place(way, k):
        return 0 if k == 0 else (2 * k - 1 if way == 0 or k == far else 2 * k)

    def goes(way, k, h):
        return k < far - 1 or (k == far - 1 and h == way)

    def spread(way, k, h):
        return remote(
            tokens_at.at[place(way, k), h],
            tokens_at.at[place(way, k + 1), h],
            tok_send.at[way, k, h],
            tok_recv.at[place(way, k + 1), h],
            s,
            right if way == 0 else left,
        )

    def start_hop(copy, k):
        for h in (0, 1):
            for way in (0, 1):
                hh = h if way == 0 else 1 - h
                if goes(way, k, hh):
                    copy(way, k, hh).start()

    def pass_on(copy, k):
        for h in (0, 1):
            for way in (0, 1):
                hh = h if way == 0 else 1 - h
                if goes(way, k - 1, hh):
                    copy(way, k - 1, hh).wait_recv()
                    if goes(way, k, hh):
                        copy(way, k, hh).start()

    def normalize(cols):
        return (resid[:, cols].astype(F32) * scale * gain_ref[:, cols]).astype(BF16)

    def set_tokens(cols):
        tokens_at[0, :, :, cols] = normalize(cols).reshape(2, ht, tile)

    column_loop(0, early, set_tokens)
    start_hop(spread, 0)

    slot_of = lax.broadcasted_iota(jnp.int32, (slots, tokens), 0).astype(F32)

    def hits(q, i):
        return slot_of == info[q, i : i + 1, :tokens]

    def chooser(q):
        return jnp.where(hits(q, 0) | hits(q, 1), 1.0, 0.0).astype(BF16)

    def weigher(q):
        share = jnp.where(hits(q, 0), info[q, 2:3, :tokens], 0.0) + jnp.where(
            hits(q, 1), info[q, 3:4, :tokens], 0.0
        )
        share = share.T
        high = share.astype(BF16)
        return high, (share - high.astype(F32)).astype(BF16)

    def choose(q, rows, cols, pick):
        chosen = jnp.dot(pick, rows, preferred_element_type=F32)
        sent[q, :, :, cols] = chosen.astype(BF16).reshape(nsp, cap, tile)

    def over_plane(src, dst, q, cols, send, recv):
        def copy(i):
            e = lax.rem(s + i, nsp)
            return remote(src.at[q, e, :, cols], dst.at[q, s, :, cols], send, recv, e, t)

        def begin(i, carry):
            copy(i).start()
            return carry

        lax.fori_loop(1, nsp, begin, 0)
        pltpu.make_async_copy(src.at[q, s, :, cols], dst.at[q, s, :, cols], recv).start()

    def all_in(dst, q, cols, recv):
        pltpu.make_async_copy(dst.at[q, :, :, cols], dst.at[q, :, :, cols], recv).wait()

    def all_out(src, q, cols, send):
        block = src.at[q, pl.ds(0, nsp - 1), :, cols]
        pltpu.make_async_copy(block, block, send).wait()

    own_pick = chooser(0)
    column_loop(early, width, lambda cols: choose(0, normalize(cols), cols, own_pick))
    over_plane(sent, x, 0, late, disp_send.at[0], disp_recv.at[0])
    column_loop(
        0, early, lambda cols: choose(0, tokens_at[0, :, :, cols].reshape(tokens, tile), cols, own_pick)
    )
    over_plane(sent, x, 0, ahead, plane_send.at[0], plane_recv.at[0])

    def tell_in(q):
        pltpu.make_async_copy(info.at[q], info.at[q], info_recv.at[q]).wait()

    def select(q):
        tell_in(q)
        pick = chooser(q)
        column_loop(
            0, early, lambda cols: choose(q, tokens_at[q, :, :, cols].reshape(tokens, tile), cols, pick)
        )
        over_plane(sent, x, q, ahead, plane_send.at[q], plane_recv.at[q])

    def q_loop(first, last, f):
        def body(q, carry):
            f(q)
            return carry

        lax.fori_loop(first, last, body, 0)

    pass_on(spread, 1)
    q_loop(1, min(3, nz), select)
    all_in(x, 0, late, disp_recv.at[0])

    def gather(way, k, h):
        return remote(
            half(x, place(way, k), h),
            half(x, place(way, k + 1), h),
            ag_send.at[way, k, h],
            ag_recv.at[place(way, k + 1), h],
            s,
            right if way == 0 else left,
        )

    def ffn(q, n):
        rows = x[pl.ds(q, n)].reshape(n * slots, width)
        filled = pl.ds(0, n * slots)
        for b in range(2):
            g = lax.dot_general(rows, gate_w[b], by_row, preferred_element_type=F32)
            u = lax.dot_general(rows, up_w[b], by_row, preferred_element_type=F32)
            hidden[b, filled] = (jax.nn.silu(g) * u).astype(BF16)

        def columns(j, carry):
            cols = pl.ds(pl.multiple_of(j * wide, wide), wide)
            acc = jnp.dot(hidden[0, filled], down_w[0, :, cols], preferred_element_type=F32)
            acc = acc + jnp.dot(hidden[1, filled], down_w[1, :, cols], preferred_element_type=F32)
            y[pl.ds(q, n), :, :, cols] = acc.astype(BF16).reshape(n, nsp, cap, wide)
            return carry

        lax.fori_loop(0, width // wide, columns, 0)

    def experts(q, n):
        for i in range(n):
            all_in(x, q + i, ahead, plane_recv.at[q + i])
        ffn(q, n)
        for i in range(n):
            over_plane(y, back_at, q + i, ahead, back_send.at[q + i], back_recv.at[q + i])

    def arm(way, r):
        k = far - r
        if k == 0 or k == far:
            return 0 if k == 0 else 2 * far - 1
        return 2 * k if way == 0 else 2 * k - 1

    landed = (from_left, from_right)

    def reduce(way, r, h):
        return remote(
            half(y, arm(way, r), h),
            half(landed[way], r, h),
            rs_send.at[way, r, h],
            rs_recv.at[way, r, h],
            s,
            right if way == 0 else left,
        )

    def moves(way, r, h):
        return r > 0 or h != way

    def open_arms(copy):
        for way in (0, 1):
            copy(way, 0, 1 - way).start()

    def second_halves(copy):
        if far > 1:
            for way in (0, 1):
                copy(way, 1, way).start()

    start_hop(gather, 0)
    for k in range(2, far + 1):
        pass_on(spread, k)
        q_loop(2 * k - 1, min(2 * k + 1, nz), select)
    for i, (src, dst) in enumerate(pairs):
        pltpu.make_async_copy(src.at[0], dst.at[0], own_sem.at[i]).wait()
    for i in range(3):
        to_mate(i).wait_recv()
    experts(0, 1)
    for k in range(1, far + 1):
        pass_on(gather, k)
        experts(2 * k - 1, 2 if k < far else 1)
        if k == far - 1:
            second_halves(reduce)

    def add(q, buf, r, h):
        rows = pl.ds(h * hs, hs)

        def body(cols):
            y[q, rows, :, cols] = (
                y[q, rows, :, cols].astype(F32) + buf[r, rows, :, cols].astype(F32)
            ).astype(BF16)

        column_loop(early, width, body)

    sums_landed = (sums_left, sums_right)

    def reduce_sums(way, r, h):
        return remote(
            sums.at[arm(way, r), h],
            sums_landed[way].at[r, h],
            sum_send.at[way, r, h],
            sum_recv.at[way, r, h],
            s,
            right if way == 0 else left,
        )

    def add_sums(q, buf, r, h):
        sums[q, h] = (sums[q, h].astype(F32) + buf[r, h].astype(F32)).astype(BF16)

    def combine(q):
        all_in(back_at, q, ahead, back_recv.at[q])
        high, low = weigher(q)

        def body(cols):
            rows = back_at[q, :, :, cols].reshape(slots, tile)
            mixed = jnp.dot(high, rows, preferred_element_type=F32)
            mixed = mixed + jnp.dot(low, rows, preferred_element_type=F32)
            sums[q, :, :, cols] = mixed.astype(BF16).reshape(2, ht, tile)

        column_loop(0, early, body)

    def advance(copy, plus, bufs, r):
        for h in (0, 1):
            for way in (0, 1):
                hh = 1 - h if way == 0 else h
                if r == 1 and hh == way:
                    continue
                copy(way, r - 1, hh).wait_recv()
                plus(arm(way, r), bufs[way], r - 1, hh)
                copy(way, r, hh).start()

    open_arms(reduce)
    q_loop(nz - 1, nz, combine)
    open_arms(reduce_sums)
    if far > 1:
        q_loop(nz - 3, nz - 1, combine)
        second_halves(reduce_sums)
    for r in range(1, far):
        advance(reduce, add, landed, r)
        if r + 1 < far:
            q_loop(nz - 3 - 2 * r, nz - 1 - 2 * r, combine)
        advance(reduce_sums, add_sums, sums_landed, r)
    q_loop(0, 1, combine)

    for h in (0, 1):
        rows = pl.ds(h * hs, hs)
        for way in (0, 1):
            if moves(way, far - 1, h):
                reduce(way, far - 1, h).wait_recv()

        def finish(cols):
            total = y[0, rows, :, cols].astype(F32)
            for way in (0, 1):
                if moves(way, far - 1, h):
                    total = total + landed[way][far - 1, rows, :, cols].astype(F32)
            final[0, rows, :, cols] = total.astype(BF16)

        column_loop(early, width, finish)

    over_plane(final, returned, 0, late, ret_send.at[0], ret_recv.at[0])

    for h in (0, 1):
        rows = pl.ds(h * ht, ht)
        for way in (0, 1):
            if moves(way, far - 1, h):
                reduce_sums(way, far - 1, h).wait_recv()

        def finish_sums(cols):
            total = resid[rows, cols].astype(F32) + sums[0, h, :, cols].astype(F32)
            for way in (0, 1):
                if moves(way, far - 1, h):
                    total = total + sums_landed[way][far - 1, h, :, cols].astype(F32)
            out_ref[rows, cols] = total.astype(BF16)

        column_loop(0, early, finish_sums)

    high, low = weigher(0)
    all_in(returned, 0, late, ret_recv.at[0])

    def finish_late(cols):
        rows = returned[0, :, :, cols].reshape(slots, tile)
        mixed = jnp.dot(high, rows, preferred_element_type=F32)
        mixed = mixed + jnp.dot(low, rows, preferred_element_type=F32)
        out_ref[:, cols] = (resid[:, cols].astype(F32) + mixed).astype(BF16)

    column_loop(early, width, finish_late)

    @pl.when(s < nsp - 1)
    def _():
        to_next().wait_send()

    def drain_conv(p, carry):
        for core in (0, 1):

            @pl.when(2 * p + core != t)
            def _():
                to_owner(p, core).wait_send()

        return carry

    lax.fori_loop(0, nz, drain_conv, 0)

    def drain_tell(i, carry):
        tell(i).wait_send()
        return carry

    lax.fori_loop(1, nz, drain_tell, 0)
    all_out(sent, 0, late, disp_send.at[0])
    all_out(final, 0, late, ret_send.at[0])

    def drain_plane(q):
        all_out(sent, q, ahead, plane_send.at[q])
        all_out(y, q, ahead, back_send.at[q])

    q_loop(0, nz, drain_plane)
    for i in range(3):
        to_mate(i).wait_send()
    for way in (0, 1):
        for k in range(far):
            for h in (0, 1):
                if goes(way, k, h):
                    gather(way, k, h).wait_send()
                    spread(way, k, h).wait_send()
                if moves(way, k, h):
                    reduce(way, k, h).wait_send()
                    reduce_sums(way, k, h).wait_send()


def per_device(
    conv_value,
    conv_gate,
    conv_taps,
    norm_gain,
    norm_bias,
    out_weight,
    stream,
    routes,
    route_weights,
    expert_gain,
    expert_gate,
    expert_up,
    expert_down,
):
    nsp, ntp = lax.axis_size("sp"), lax.axis_size("tp")
    nz = ntp // 2
    tokens, width = stream.shape
    local_ch, taps = conv_taps.shape
    sub = local_ch // 2
    hid = expert_gate.shape[2]
    cap = 2 * tokens // nsp
    far = nz // 2
    lanes = 2 * tokens
    group = ntp * sub
    early = width // 2
    vmem = pl.BlockSpec(memory_space=pltpu.VMEM)
    hbm = pl.BlockSpec(memory_space=pl.ANY)
    dma = pltpu.SemaphoreType.DMA
    return pl.pallas_call(
        functools.partial(kernel, nsp, nz, early),
        out_shape=pltpu.VMEM((tokens, width), BF16),
        in_specs=[vmem] * 5 + [hbm] * 2 + [vmem] * 3 + [hbm] * 3,
        out_specs=vmem,
        scratch_shapes=[
            pltpu.VMEM((nz + 1, local_ch, lanes), F32),
            pltpu.VMEM((taps, local_ch, lanes), F32),
            pltpu.VMEM((local_ch, lanes), BF16),
            pltpu.VMEM((local_ch, lanes), BF16),
            pltpu.VMEM((nz, 2, sub, lanes), BF16),
            pltpu.VMEM((ntp, sub, lanes), BF16),
            pltpu.VMEM((2, tokens, group), BF16),
            pltpu.VMEM((2, ntp, sub, width), BF16),
            pltpu.VMEM((tokens, width), BF16),
            pltpu.VMEM((tokens, width), BF16),
            pltpu.VMEM((2, hid, width), BF16),
            pltpu.VMEM((2, hid, width), BF16),
            pltpu.VMEM((2, hid, width), BF16),
            pltpu.VMEM((2, 2 * nsp * cap, hid), BF16),
            pltpu.VMEM((nz, 8, lanes), F32),
            pltpu.VMEM((nz, 2, tokens // 2, early), BF16),
            pltpu.VMEM((nz, nsp, cap, width), BF16),
            pltpu.VMEM((nz, nsp, cap, width), BF16),
            pltpu.VMEM((nz, nsp, cap, width), BF16),
            pltpu.VMEM((nz, nsp, cap, early), BF16),
            pltpu.VMEM((nz, 2, tokens // 2, early), BF16),
            pltpu.VMEM((far, nsp, cap, width), BF16),
            pltpu.VMEM((far, nsp, cap, width), BF16),
            pltpu.VMEM((far, 2, tokens // 2, early), BF16),
            pltpu.VMEM((far, 2, tokens // 2, early), BF16),
            pltpu.VMEM((1, nsp, cap, width), BF16),
            pltpu.VMEM((1, nsp, cap, width), BF16),
            dma((3,)),
            dma((1,)),
            dma((1,)),
            dma((nz, 2)),
            dma((ntp,)),
            dma((3,)),
            dma((3,)),
            dma((3,)),
            dma((nz,)),
            dma((nz,)),
            dma((1,)),
            dma((1,)),
            dma((nz,)),
            dma((nz,)),
            dma((2, far, 2)),
            dma((nz, 2)),
            dma((2, far, 2)),
            dma((nz, 2)),
            dma((2, far, 2)),
            dma((2, far, 2)),
            dma((2, far, 2)),
            dma((2, far, 2)),
            dma((nz,)),
            dma((nz,)),
            dma((1,)),
            dma((1,)),
        ],
        compiler_params=pltpu.CompilerParams(
            collective_id=0, has_side_effects=True, vmem_limit_bytes=60 * 1024 * 1024
        ),
        name="block",
    )(
        conv_value,
        conv_gate,
        conv_taps.T,
        norm_gain[None, :],
        norm_bias[None, :],
        out_weight.reshape(ntp, 2, sub, width),
        stream,
        routes.T,
        route_weights.T,
        expert_gain[None, :],
        expert_gate.swapaxes(1, 2),
        expert_up.swapaxes(1, 2),
        expert_down,
    )


def solution(mesh):
    return jax.shard_map(
        per_device,
        mesh=mesh,
        in_specs=(
            P("tp", "sp"),
            P("tp", "sp"),
            P("tp", None),
            P(),
            P(),
            P(),
            P(("sp", "tp"), None),
            P(("sp", "tp"), None),
            P(("sp", "tp"), None),
            P(),
            P("sp", None, "tp"),
            P("sp", None, "tp"),
            P("sp", "tp", None),
        ),
        out_specs=P(("sp", "tp"), None),
        check_vma=False,
    )
```

```python
import functools

import jax
import jax.numpy as jnp
from jax import lax
from jax.experimental import pallas as pl
from jax.experimental.pallas import tpu as pltpu
from jax.sharding import PartitionSpec as P

epsilon = 1e-06
BF16 = jnp.bfloat16
F32 = jnp.float32
MESH = pl.DeviceIdType.MESH
by_row = (((1,), (1,)), ((), ()))


def kernel(
    nsp,
    nz,
    early,
    value_ref,
    gating_ref,
    taps_ref,
    norm_gain_ref,
    norm_bias_ref,
    out_w_ref,
    stream_ref,
    routes_ref,
    weights_ref,
    gain_ref,
    gate_ref,
    up_ref,
    down_ref,
    out_ref,
    gated,
    spread_taps,
    edge,
    rim,
    conv_out,
    conv_in,
    act,
    out_w,
    stream,
    resid,
    gate_w,
    up_w,
    down_w,
    hidden,
    info,
    tokens_at,
    sent,
    x,
    y,
    back_at,
    sums,
    from_left,
    from_right,
    sums_left,
    sums_right,
    final,
    returned,
    in_sem,
    rim_send,
    rim_recv,
    conv_send,
    conv_recv,
    own_sem,
    mate_send,
    mate_recv,
    info_send,
    info_recv,
    disp_send,
    disp_recv,
    plane_send,
    plane_recv,
    tok_send,
    tok_recv,
    ag_send,
    ag_recv,
    rs_send,
    rs_recv,
    sum_send,
    sum_recv,
    back_send,
    back_recv,
    ret_send,
    ret_recv,
):
    s = lax.axis_index("sp")
    t = lax.axis_index("tp")
    z = lax.div(t, 2)
    c = lax.rem(t, 2)
    far = nz // 2
    hs = nsp // 2
    right = lax.rem(z + 1, nz) * 2 + c
    left = lax.rem(z + nz - 1, nz) * 2 + c
    mate = z * 2 + 1 - c
    cap = sent.shape[2]
    width = sent.shape[3]
    tokens = routes_ref.shape[1]
    slots = nsp * cap
    shift = cap.bit_length() - 1
    local_ch, run_len = value_ref.shape
    taps = taps_ref.shape[0]
    lanes = 2 * tokens
    sub = local_ch // 2
    group = act.shape[2]
    channels = 2 * group
    tile = min(512, early)
    wide = min(512, width)
    ht = tokens // 2
    late = pl.ds(early, width - early)
    ahead = pl.ds(0, early)

    def half(ref, q, h):
        return ref.at[q, pl.ds(h * hs, hs), :, late]

    def column_loop(first, last, body):
        def step(j, carry):
            body(pl.ds(pl.multiple_of(j * tile, tile), tile))
            return carry

        lax.fori_loop(first // tile, last // tile, step, 0)

    def remote(src, dst, send, recv, sp, tp):
        return pltpu.make_async_remote_copy(
            src_ref=src,
            dst_ref=dst,
            send_sem=send,
            recv_sem=recv,
            device_id={"sp": sp, "tp": tp},
            device_id_type=MESH,
        )

    loads = [
        pltpu.make_async_copy(out_w_ref.at[:, 0], out_w.at[0], in_sem.at[0]),
        pltpu.make_async_copy(out_w_ref.at[:, 1], out_w.at[1], in_sem.at[1]),
        pltpu.make_async_copy(stream_ref, stream, in_sem.at[2]),
    ]
    for load in loads:
        load.start()
    pairs = ((gate_ref, gate_w), (up_ref, up_w), (down_ref, down_w))
    for i, (src, dst) in enumerate(pairs):
        pltpu.make_async_copy(src.at[0], dst.at[0], own_sem.at[i]).start()

    barrier = pltpu.get_barrier_semaphore()

    def greet_sp(i, carry):
        pl.semaphore_signal(
            barrier,
            inc=1,
            device_id={"sp": lax.rem(s + i, nsp), "tp": t},
            device_id_type=MESH,
        )
        return carry

    def greet_tp(i, carry):
        pl.semaphore_signal(
            barrier,
            inc=1,
            device_id={"sp": s, "tp": lax.rem(t + i, 2 * nz)},
            device_id_type=MESH,
        )
        return carry

    lax.fori_loop(1, nsp, greet_sp, 0)
    lax.fori_loop(1, 2 * nz, greet_tp, 0)

    for p in range(nz - 1, -1, -1):
        cols = slice(p * lanes, (p + 1) * lanes)
        product = value_ref[:, cols].astype(F32) * jax.nn.sigmoid(gating_ref[:, cols].astype(F32))
        if p == nz - 1:
            edge[...] = product.astype(BF16)
        gated[p + 1] = product.astype(BF16).astype(F32)
    by_channel = taps_ref[...].T
    for j in range(taps):
        spread_taps[j] = jnp.broadcast_to(by_channel[:, j : j + 1], (local_ch, lanes))

    slot = lax.broadcasted_iota(jnp.int32, (slots, tokens), 0)
    expert = lax.shift_right_logical(slot, shift)
    first = routes_ref[0:1, :] == expert
    second = routes_ref[1:2, :] == expert
    named = first | second
    before = lax.broadcasted_iota(jnp.int32, (tokens, tokens), 0) < lax.broadcasted_iota(
        jnp.int32, (tokens, tokens), 1
    )
    rank = jnp.dot(
        jnp.where(named, 1.0, 0.0).astype(BF16),
        jnp.where(before, 1.0, 0.0).astype(BF16),
        preferred_element_type=F32,
    )
    pick = named & (rank == (slot & (cap - 1)).astype(F32))
    number = slot.astype(F32)
    info[0] = jnp.zeros((8, lanes), F32)
    for i, hit in enumerate((first, second)):
        info[0, i : i + 1, :tokens] = jnp.sum(
            jnp.where(hit & pick, number, 0.0), axis=0, keepdims=True
        )
        info[0, 2 + i : 3 + i, :tokens] = weights_ref[i : i + 1, :]

    def regroup(ref, h):
        return jnp.concatenate(
            [ref[:, pl.ds((2 * i + h) * sub, sub)] for i in range(2 * nz)], axis=1
        )

    affine = [(regroup(norm_gain_ref, h), regroup(norm_bias_ref, h)) for h in (0, 1)]

    pl.semaphore_wait(barrier, nsp + 2 * nz - 2)

    def to_next():
        return remote(edge, rim, rim_send.at[0], rim_recv.at[0], lax.rem(s + 1, nsp), t)

    @pl.when(s < nsp - 1)
    def _():
        to_next().start()

    def tell(i):
        q = jnp.where(i <= far, 2 * i - 1, 2 * (nz - i))
        return remote(
            info.at[0], info.at[q], info_send.at[i], info_recv.at[q], s, lax.rem(z + i, nz) * 2 + c
        )

    def start_tell(i, carry):
        tell(i).start()
        return carry

    lax.fori_loop(1, nz, start_tell, 0)

    def to_owner(p, core):
        return remote(
            conv_out.at[p, core], conv_in.at[t], conv_send.at[p, core], conv_recv.at[t], s, 2 * p + core
        )

    def stays(p, core):
        return pltpu.make_async_copy(conv_out.at[p, core], conv_in.at[t], conv_recv.at[t])

    lane = lax.broadcasted_iota(jnp.int32, (local_ch, lanes), 1)
    low_lanes = lax.broadcasted_iota(jnp.int32, (sub, lanes), 1) < tokens

    def conv_tile(i, carry):
        p = jnp.where(i == nz - 1, 0, 1 + lax.rem(z + i, nz - 1))

        @pl.when(p == 0)
        def _():
            @pl.when(s > 0)
            def _():
                to_next().wait_recv()
                gated[0] = rim[...].astype(F32)

            @pl.when(s == 0)
            def _():
                gated[0] = jnp.zeros((local_ch, lanes), F32)

        here, before = gated[p + 1], gated[p]
        total = spread_taps[taps - 1] * here
        for d in range(1, taps):
            window = pltpu.roll(jnp.where(lane >= lanes - d, before, here), d, 1)
            total = total + spread_taps[taps - 1 - d] * window
        top, bottom = total[:sub], total[sub:]
        conv_out[p, 0] = jnp.where(low_lanes, top, pltpu.roll(bottom, tokens, 1)).astype(BF16)
        conv_out[p, 1] = jnp.where(low_lanes, pltpu.roll(top, tokens, 1), bottom).astype(BF16)
        for core in (0, 1):

            @pl.when(2 * p + core != t)
            def _():
                to_owner(p, core).start()

            @pl.when(2 * p + core == t)
            def _():
                stays(p, core).start()

        return carry

    lax.fori_loop(0, nz, conv_tile, 0)

    def to_mate(i):
        src, dst = pairs[i]
        return remote(src.at[0], dst.at[1], mate_send.at[i], mate_recv.at[i], s, mate)

    for i in range(3):
        to_mate(i).start()

    def wait_conv(i, carry):
        @pl.when(i != t)
        def _():
            remote(
                conv_out.at[0, 0], conv_in.at[i], conv_send.at[0, 0], conv_recv.at[i], s, i
            ).wait_recv()

        @pl.when(i == t)
        def _():
            stays(z, 0).wait()

        return carry

    lax.fori_loop(0, 2 * nz, wait_conv, 0)

    def over_channels(value):
        part = jnp.sum(value, axis=0, keepdims=True)
        return (part + pltpu.roll(part, tokens, 1)) * (1.0 / channels)

    whole = conv_in[...].reshape(group, lanes).astype(F32)
    deviation = whole - over_channels(whole)
    spread = over_channels(deviation * deviation)
    scaled = (deviation * lax.rsqrt(spread + epsilon)).T
    for h in (0, 1):
        part = scaled[h * tokens : (h + 1) * tokens]
        act[h] = jax.nn.silu(part * affine[h][0] + affine[h][1]).astype(
            BF16
        )
    for load in loads:
        load.wait()

    def project(j, squares):
        cols = pl.ds(pl.multiple_of(j * tile, tile), tile)
        acc = stream[:, cols].astype(F32)
        for h in (0, 1):
            acc = acc + jnp.dot(
                act[h], out_w[h, :, :, cols].reshape(group, tile), preferred_element_type=F32
            )
        rounded = acc.astype(BF16)
        resid[:, cols] = rounded
        wide = rounded.astype(F32)
        return squares + jnp.sum(wide * wide, axis=1, keepdims=True)

    squares = lax.fori_loop(0, width // tile, project, jnp.zeros((tokens, 1), F32))
    scale = lax.rsqrt(squares * (1.0 / width) + epsilon)

    def place(way, k):
        return 0 if k == 0 else (2 * k - 1 if way == 0 or k == far else 2 * k)

    def goes(way, k, h):
        return k < far - 1 or (k == far - 1 and h == way)

    def spread(way, k, h):
        return remote(
            tokens_at.at[place(way, k), h],
            tokens_at.at[place(way, k + 1), h],
            tok_send.at[way, k, h],
            tok_recv.at[place(way, k + 1), h],
            s,
            right if way == 0 else left,
        )

    def start_hop(copy, k):
        for h in (0, 1):
            for way in (0, 1):
                hh = h if way == 0 else 1 - h
                if goes(way, k, hh):
                    copy(way, k, hh).start()

    def pass_on(copy, k):
        for h in (0, 1):
            for way in (0, 1):
                hh = h if way == 0 else 1 - h
                if goes(way, k - 1, hh):
                    copy(way, k - 1, hh).wait_recv()
                    if goes(way, k, hh):
                        copy(way, k, hh).start()

    def normalize(cols):
        return (resid[:, cols].astype(F32) * scale * gain_ref[:, cols]).astype(BF16)

    def set_tokens(cols):
        tokens_at[0, :, :, cols] = normalize(cols).reshape(2, ht, tile)

    column_loop(0, early, set_tokens)
    start_hop(spread, 0)

    slot_of = lax.broadcasted_iota(jnp.int32, (slots, tokens), 0).astype(F32)

    def hits(q, i):
        return slot_of == info[q, i : i + 1, :tokens]

    def chooser(q):
        return jnp.where(hits(q, 0) | hits(q, 1), 1.0, 0.0).astype(BF16)

    def weigher(q):
        share = jnp.where(hits(q, 0), info[q, 2:3, :tokens], 0.0) + jnp.where(
            hits(q, 1), info[q, 3:4, :tokens], 0.0
        )
        share = share.T
        high = share.astype(BF16)
        return high, (share - high.astype(F32)).astype(BF16)

    def choose(q, rows, cols, pick):
        chosen = jnp.dot(pick, rows, preferred_element_type=F32)
        sent[q, :, :, cols] = chosen.astype(BF16).reshape(nsp, cap, tile)

    def over_plane(src, dst, q, cols, send, recv):
        def copy(i):
            e = lax.rem(s + i, nsp)
            return remote(src.at[q, e, :, cols], dst.at[q, s, :, cols], send, recv, e, t)

        def begin(i, carry):
            copy(i).start()
            return carry

        lax.fori_loop(1, nsp, begin, 0)
        pltpu.make_async_copy(src.at[q, s, :, cols], dst.at[q, s, :, cols], recv).start()

    def all_in(dst, q, cols, recv):
        pltpu.make_async_copy(dst.at[q, :, :, cols], dst.at[q, :, :, cols], recv).wait()

    def all_out(src, q, cols, send):
        block = src.at[q, pl.ds(0, nsp - 1), :, cols]
        pltpu.make_async_copy(block, block, send).wait()

    own_pick = chooser(0)
    column_loop(early, width, lambda cols: choose(0, normalize(cols), cols, own_pick))
    over_plane(sent, x, 0, late, disp_send.at[0], disp_recv.at[0])
    column_loop(
        0, early, lambda cols: choose(0, tokens_at[0, :, :, cols].reshape(tokens, tile), cols, own_pick)
    )
    over_plane(sent, x, 0, ahead, plane_send.at[0], plane_recv.at[0])

    def tell_in(q):
        pltpu.make_async_copy(info.at[q], info.at[q], info_recv.at[q]).wait()

    def select(q):
        tell_in(q)
        pick = chooser(q)
        column_loop(
            0, early, lambda cols: choose(q, tokens_at[q, :, :, cols].reshape(tokens, tile), cols, pick)
        )
        over_plane(sent, x, q, ahead, plane_send.at[q], plane_recv.at[q])

    def q_loop(first, last, f):
        def body(q, carry):
            f(q)
            return carry

        lax.fori_loop(first, last, body, 0)

    pass_on(spread, 1)
    q_loop(1, min(3, nz), select)
    all_in(x, 0, late, disp_recv.at[0])

    def gather(way, k, h):
        return remote(
            half(x, place(way, k), h),
            half(x, place(way, k + 1), h),
            ag_send.at[way, k, h],
            ag_recv.at[place(way, k + 1), h],
            s,
            right if way == 0 else left,
        )

    def ffn(q, n):
        rows = x[pl.ds(q, n)].reshape(n * slots, width)
        filled = pl.ds(0, n * slots)
        for b in range(2):
            g = lax.dot_general(rows, gate_w[b], by_row, preferred_element_type=F32)
            u = lax.dot_general(rows, up_w[b], by_row, preferred_element_type=F32)
            hidden[b, filled] = (jax.nn.silu(g) * u).astype(BF16)

        def columns(j, carry):
            cols = pl.ds(pl.multiple_of(j * wide, wide), wide)
            acc = jnp.dot(hidden[0, filled], down_w[0, :, cols], preferred_element_type=F32)
            acc = acc + jnp.dot(hidden[1, filled], down_w[1, :, cols], preferred_element_type=F32)
            y[pl.ds(q, n), :, :, cols] = acc.astype(BF16).reshape(n, nsp, cap, wide)
            return carry

        lax.fori_loop(0, width // wide, columns, 0)

    def experts(q, n):
        for i in range(n):
            all_in(x, q + i, ahead, plane_recv.at[q + i])
        ffn(q, n)
        for i in range(n):
            over_plane(y, back_at, q + i, ahead, back_send.at[q + i], back_recv.at[q + i])

    def arm(way, r):
        k = far - r
        if k == 0 or k == far:
            return 0 if k == 0 else 2 * far - 1
        return 2 * k if way == 0 else 2 * k - 1

    landed = (from_left, from_right)

    def reduce(way, r, h):
        return remote(
            half(y, arm(way, r), h),
            half(landed[way], r, h),
            rs_send.at[way, r, h],
            rs_recv.at[way, r, h],
            s,
            right if way == 0 else left,
        )

    def moves(way, r, h):
        return r > 0 or h != way

    def open_arms(copy):
        for way in (0, 1):
            copy(way, 0, 1 - way).start()

    def second_halves(copy):
        if far > 1:
            for way in (0, 1):
                copy(way, 1, way).start()

    start_hop(gather, 0)
    def spread_and_select(k):
        if k <= far:
            pass_on(spread, k)
            q_loop(2 * k - 1, min(2 * k + 1, nz), select)

    spread_and_select(2)
    for i, (src, dst) in enumerate(pairs):
        pltpu.make_async_copy(src.at[0], dst.at[0], own_sem.at[i]).wait()
    for i in range(3):
        to_mate(i).wait_recv()
    experts(0, 1)
    for k in range(1, far + 1):
        pass_on(gather, k)
        spread_and_select(k + 2)
        experts(2 * k - 1, 2 if k < far else 1)
        if k == far - 1:
            second_halves(reduce)

    def add(q, buf, r, h):
        rows = pl.ds(h * hs, hs)

        def body(cols):
            y[q, rows, :, cols] = (
                y[q, rows, :, cols].astype(F32) + buf[r, rows, :, cols].astype(F32)
            ).astype(BF16)

        column_loop(early, width, body)

    sums_landed = (sums_left, sums_right)

    def reduce_sums(way, r, h):
        return remote(
            sums.at[arm(way, r), h],
            sums_landed[way].at[r, h],
            sum_send.at[way, r, h],
            sum_recv.at[way, r, h],
            s,
            right if way == 0 else left,
        )

    def add_sums(q, buf, r, h):
        sums[q, h] = (sums[q, h].astype(F32) + buf[r, h].astype(F32)).astype(BF16)

    def combine(q):
        all_in(back_at, q, ahead, back_recv.at[q])
        high, low = weigher(q)

        def body(cols):
            rows = back_at[q, :, :, cols].reshape(slots, tile)
            mixed = jnp.dot(high, rows, preferred_element_type=F32)
            mixed = mixed + jnp.dot(low, rows, preferred_element_type=F32)
            sums[q, :, :, cols] = mixed.astype(BF16).reshape(2, ht, tile)

        column_loop(0, early, body)

    def advance(copy, plus, bufs, r):
        for h in (0, 1):
            for way in (0, 1):
                hh = 1 - h if way == 0 else h
                if r == 1 and hh == way:
                    continue
                copy(way, r - 1, hh).wait_recv()
                plus(arm(way, r), bufs[way], r - 1, hh)
                copy(way, r, hh).start()

    def finish_reduce():
        for h in (0, 1):
            rows = pl.ds(h * hs, hs)
            for way in (0, 1):
                if moves(way, far - 1, h):
                    reduce(way, far - 1, h).wait_recv()

            def finish(cols):
                total = y[0, rows, :, cols].astype(F32)
                for way in (0, 1):
                    if moves(way, far - 1, h):
                        total = total + landed[way][far - 1, rows, :, cols].astype(F32)
                final[0, rows, :, cols] = total.astype(BF16)

            column_loop(early, width, finish)

        over_plane(final, returned, 0, late, ret_send.at[0], ret_recv.at[0])

    open_arms(reduce)
    if far > 1:
        advance(reduce, add, landed, 1)
    q_loop(nz - 1, nz, combine)
    open_arms(reduce_sums)
    if far > 1:
        q_loop(nz - 3, nz - 1, combine)
        second_halves(reduce_sums)
    for r in range(1, far):
        if r + 1 < far:
            advance(reduce, add, landed, r + 1)
            q_loop(nz - 3 - 2 * r, nz - 1 - 2 * r, combine)
        else:
            q_loop(0, 1, combine)
            finish_reduce()
        advance(reduce_sums, add_sums, sums_landed, r)
    if far == 1:
        q_loop(0, 1, combine)
        finish_reduce()


    for h in (0, 1):
        rows = pl.ds(h * ht, ht)
        for way in (0, 1):
            if moves(way, far - 1, h):
                reduce_sums(way, far - 1, h).wait_recv()

        def finish_sums(cols):
            total = resid[rows, cols].astype(F32) + sums[0, h, :, cols].astype(F32)
            for way in (0, 1):
                if moves(way, far - 1, h):
                    total = total + sums_landed[way][far - 1, h, :, cols].astype(F32)
            out_ref[rows, cols] = total.astype(BF16)

        column_loop(0, early, finish_sums)

    high, low = weigher(0)
    all_in(returned, 0, late, ret_recv.at[0])

    def finish_late(cols):
        rows = returned[0, :, :, cols].reshape(slots, tile)
        mixed = jnp.dot(high, rows, preferred_element_type=F32)
        mixed = mixed + jnp.dot(low, rows, preferred_element_type=F32)
        out_ref[:, cols] = (resid[:, cols].astype(F32) + mixed).astype(BF16)

    column_loop(early, width, finish_late)

    @pl.when(s < nsp - 1)
    def _():
        to_next().wait_send()

    def drain_conv(p, carry):
        for core in (0, 1):

            @pl.when(2 * p + core != t)
            def _():
                to_owner(p, core).wait_send()

        return carry

    lax.fori_loop(0, nz, drain_conv, 0)

    def drain_tell(i, carry):
        tell(i).wait_send()
        return carry

    lax.fori_loop(1, nz, drain_tell, 0)
    all_out(sent, 0, late, disp_send.at[0])
    all_out(final, 0, late, ret_send.at[0])

    def drain_plane(q):
        all_out(sent, q, ahead, plane_send.at[q])
        all_out(y, q, ahead, back_send.at[q])

    q_loop(0, nz, drain_plane)
    for i in range(3):
        to_mate(i).wait_send()
    for way in (0, 1):
        for k in range(far):
            for h in (0, 1):
                if goes(way, k, h):
                    gather(way, k, h).wait_send()
                    spread(way, k, h).wait_send()
                if moves(way, k, h):
                    reduce(way, k, h).wait_send()
                    reduce_sums(way, k, h).wait_send()


def per_device(
    conv_value,
    conv_gate,
    conv_taps,
    norm_gain,
    norm_bias,
    out_weight,
    stream,
    routes,
    route_weights,
    expert_gain,
    expert_gate,
    expert_up,
    expert_down,
):
    nsp, ntp = lax.axis_size("sp"), lax.axis_size("tp")
    nz = ntp // 2
    tokens, width = stream.shape
    local_ch, taps = conv_taps.shape
    sub = local_ch // 2
    hid = expert_gate.shape[2]
    cap = 2 * tokens // nsp
    far = nz // 2
    lanes = 2 * tokens
    group = ntp * sub
    early = width // 2
    vmem = pl.BlockSpec(memory_space=pltpu.VMEM)
    hbm = pl.BlockSpec(memory_space=pl.ANY)
    dma = pltpu.SemaphoreType.DMA
    return pl.pallas_call(
        functools.partial(kernel, nsp, nz, early),
        out_shape=pltpu.VMEM((tokens, width), BF16),
        in_specs=[vmem] * 5 + [hbm] * 2 + [vmem] * 3 + [hbm] * 3,
        out_specs=vmem,
        scratch_shapes=[
            pltpu.VMEM((nz + 1, local_ch, lanes), F32),
            pltpu.VMEM((taps, local_ch, lanes), F32),
            pltpu.VMEM((local_ch, lanes), BF16),
            pltpu.VMEM((local_ch, lanes), BF16),
            pltpu.VMEM((nz, 2, sub, lanes), BF16),
            pltpu.VMEM((ntp, sub, lanes), BF16),
            pltpu.VMEM((2, tokens, group), BF16),
            pltpu.VMEM((2, ntp, sub, width), BF16),
            pltpu.VMEM((tokens, width), BF16),
            pltpu.VMEM((tokens, width), BF16),
            pltpu.VMEM((2, hid, width), BF16),
            pltpu.VMEM((2, hid, width), BF16),
            pltpu.VMEM((2, hid, width), BF16),
            pltpu.VMEM((2, 2 * nsp * cap, hid), BF16),
            pltpu.VMEM((nz, 8, lanes), F32),
            pltpu.VMEM((nz, 2, tokens // 2, early), BF16),
            pltpu.VMEM((nz, nsp, cap, width), BF16),
            pltpu.VMEM((nz, nsp, cap, width), BF16),
            pltpu.VMEM((nz, nsp, cap, width), BF16),
            pltpu.VMEM((nz, nsp, cap, early), BF16),
            pltpu.VMEM((nz, 2, tokens // 2, early), BF16),
            pltpu.VMEM((far, nsp, cap, width), BF16),
            pltpu.VMEM((far, nsp, cap, width), BF16),
            pltpu.VMEM((far, 2, tokens // 2, early), BF16),
            pltpu.VMEM((far, 2, tokens // 2, early), BF16),
            pltpu.VMEM((1, nsp, cap, width), BF16),
            pltpu.VMEM((1, nsp, cap, width), BF16),
            dma((3,)),
            dma((1,)),
            dma((1,)),
            dma((nz, 2)),
            dma((ntp,)),
            dma((3,)),
            dma((3,)),
            dma((3,)),
            dma((nz,)),
            dma((nz,)),
            dma((1,)),
            dma((1,)),
            dma((nz,)),
            dma((nz,)),
            dma((2, far, 2)),
            dma((nz, 2)),
            dma((2, far, 2)),
            dma((nz, 2)),
            dma((2, far, 2)),
            dma((2, far, 2)),
            dma((2, far, 2)),
            dma((2, far, 2)),
            dma((nz,)),
            dma((nz,)),
            dma((1,)),
            dma((1,)),
        ],
        compiler_params=pltpu.CompilerParams(
            collective_id=0, has_side_effects=True, vmem_limit_bytes=60 * 1024 * 1024
        ),
        name="block",
    )(
        conv_value,
        conv_gate,
        conv_taps.T,
        norm_gain[None, :],
        norm_bias[None, :],
        out_weight.reshape(ntp, 2, sub, width),
        stream,
        routes.T,
        route_weights.T,
        expert_gain[None, :],
        expert_gate.swapaxes(1, 2),
        expert_up.swapaxes(1, 2),
        expert_down,
    )


def solution(mesh):
    return jax.shard_map(
        per_device,
        mesh=mesh,
        in_specs=(
            P("tp", "sp"),
            P("tp", "sp"),
            P("tp", None),
            P(),
            P(),
            P(),
            P(("sp", "tp"), None),
            P(("sp", "tp"), None),
            P(("sp", "tp"), None),
            P(),
            P("sp", None, "tp"),
            P("sp", None, "tp"),
            P("sp", "tp", None),
        ),
        out_specs=P(("sp", "tp"), None),
        check_vma=False,
    )
```
